32 devices in a mesh: sp: 8 (over z, core), tp: 4 (over y, x).
Axes of the slice: x: 2, y: 2, z: 4, core: 2. Of those that a mesh axis runs over, the one named last changes fastest.
Arguments:
- cell_query_heads: bfloat16 [1024, 2048], P('sp', 'tp'), may hold values from -6 to 6
- cell_key_heads: bfloat16 [1024, 2048], P('sp', 'tp'), may hold values from -6 to 6
- cell_value_heads: bfloat16 [1024, 2048], P('sp', 'tp'), may hold values from -6 to 6
- output_gate_logits: bfloat16 [1024, 2048], P('sp', 'tp'), may hold values from -6 to 6
- input_gate_log: float32 [1024, 16], P('sp', 'tp'), may hold values from -7 to 310
- forget_gate_logits: float32 [1024, 16], P('sp', 'tp'), may hold values from 1 to 14
- extra_log_decay: float32 [1024, 16], P('sp', 'tp'), may hold values from -1 to 0
- documents: int32 [1024], P('sp'), may hold values from 0 to 7, never falling along the last dimension, each value on 1 to 256 neighbouring positions
- head_norm_gain: float32 [2048], P('tp'), may hold values from 0.1 to 1.9
- stream: bfloat16 [1024, 4096], P('sp', 'tp'), may hold values from -6 to 6
- output_weight: bfloat16 [2048, 4096], P(None, 'tp'), may hold values from -0.125 to 0.125
- expert_norm_gain: bfloat16 [4096], P('tp'), may hold values from 0.099609375 to 1.8984375
- expert_choice_index: int32 [1024, 2], P('sp'), may hold values from 0 to 7, all different within a row; in each aligned block of 128 rows (0 to 127, 128 to 255, ...) at most 64 rows name the same one
- routing_weight: float32 [1024, 2], P('sp'), may hold values from 0.2 to 1
- gate_weight: bfloat16 [8, 4096, 2048], P('sp', None, 'tp'), may hold values from -0.09375 to 0.09375
- up_weight: bfloat16 [8, 4096, 2048], P('sp', None, 'tp'), may hold values from -0.09375 to 0.09375
- down_weight: bfloat16 [8, 2048, 4096], P('sp', None, 'tp'), may hold values from -0.125 to 0.125
Outputs:
- output: bfloat16 [1024, 4096], P('sp', 'tp')
The draws below stay inside these ranges and needn't reach their ends.
Inputs may be any that keep to these rules, and one draw needn't show every extreme that they name: `expert_choice_index`: in the rows of one index of sp no expert is named more than 64 times, a bound that some block reaches. `documents`: never falling; each document 1 to 256 positions, one exactly 256.
All inputs are finite; a program needn't handle non-finite values.
Results may differ from the reference program's by a relative error of at most 0.01.
Values may be sent and summed in bfloat16 or wider, within the bound.
A program may use at most 64 MiB of HBM per device.

```python
import math
import jax
import jax.numpy as jnp
import numpy as np
from jax import lax

D = 4096
CELL_HEADS = 16
HD = 128
FF = 2048
TOPK = 2
TOKENS_PER_SHARD = 128
DOCS = 8
SEQ = 1024
EXPERTS = 8
CAP = 64
DOC_MOST = 256
N_SP = 8


def draw_forget_gate_logits(key, part):
    head_key = jax.random.fold_in(key, 11)
    block_key = jax.random.fold_in(key, 12)
    noise_key = jax.random.fold_in(key, 13)
    fast_heads = jax.random.randint(head_key, (CELL_HEADS,), 0, 2) == 0
    level = jnp.where(fast_heads, jnp.log(40.0), jnp.log(SEQ / 1.5)).astype(jnp.float32)
    block_list = SEQ // TOKENS_PER_SHARD
    shift = jax.random.uniform(block_key, (block_list, 1, CELL_HEADS), jnp.float32, -0.7, 0.7)
    noise = 0.5 * jnp.clip(jax.random.normal(noise_key, (block_list, TOKENS_PER_SHARD, CELL_HEADS), jnp.float32), -3.0, 3.0)
    return (level[None, None, :] + shift + noise).reshape(SEQ, CELL_HEADS)


def draw_input_gate_log(key, part):
    base_key = jax.random.fold_in(key, 21)
    values = jnp.clip(jax.random.normal(base_key, (SEQ, CELL_HEADS), jnp.float32), -6.0, 6.0)
    return values


def draw_extra_log_decay(key, part):
    mark_key = jax.random.fold_in(key, 31)
    depth_key = jax.random.fold_in(key, 32)
    marks = jax.random.randint(mark_key, (SEQ, CELL_HEADS), 0, SEQ // 8) == 0
    depth = jax.random.uniform(depth_key, (SEQ, CELL_HEADS), jnp.float32, jnp.log(0.5), jnp.log(0.8))
    return jnp.where(marks, depth, 0.0).astype(jnp.float32)


def shard_levels(key, dims, pieces, smallest, high):
    level, own = 1.0, jax.random.fold_in(key, 6)
    for axis_at, parts in pieces:
        draws = jnp.exp(jax.random.uniform(jax.random.fold_in(own, axis_at), (parts,), jnp.float32, smallest / len(pieces), high / len(pieces)))
        level = level * jnp.repeat(draws, dims[axis_at] // parts).reshape([-1 if axis == axis_at else 1 for axis in range(len(dims))])
    return level


def length_profile(count, total, reach, slope):
    portions = [(1 << 20) // math.isqrt(rank ** slope) + 1 for rank in range(2, count + 1)]
    surplus, given = total - reach - (count - 1), [1] * (count - 1)
    while surplus > 0:
        free = [i for i in range(count - 1) if given[i] < reach]
        pool, left = sum([portions[i] for i in free]), surplus
        for i in free:
            extra = min(reach - given[i], max(1, left * portions[i] // pool), surplus)
            given[i] = given[i] + extra
            surplus = surplus - extra
    return np.array([reach] + given)


def ragged(own_key, number_of, total, limit, skew):
    if number_of == 2:
        one = jax.random.randint(own_key, (), max(1, total - limit), min(limit, total - 1) + 1)
        return jnp.stack([one, total - one])
    lengths = jnp.asarray(length_profile(number_of, total, limit, skew), jnp.int32)
    pairs = (number_of - 1) // 2
    giver, taker = lengths[1:1 + 2 * pairs:2], lengths[2:2 + 2 * pairs:2]
    margin = jnp.minimum(giver - 1, limit - taker)
    passed = jax.random.randint(jax.random.fold_in(own_key, 1), (pairs,), 0, 1 << 20) % (margin + 1)
    lengths = lengths.at[1:1 + 2 * pairs:2].set(giver - passed).at[2:2 + 2 * pairs:2].set(taker + passed)
    return lengths[jax.random.permutation(jax.random.fold_in(own_key, 2), number_of)]


def assign_block(stream_key, own, number, rows, number_of, top, most, lean):
    sequence = jax.random.permutation(stream_key, number_of)
    heavy_load, common = portions_of(number_of, rows * top, most, lean, True), portions_of(number_of, rows * top, most, lean, False)
    places = jnp.arange(number_of)

    def named(tallies, rotation):
        used = int((tallies > 0).sum())
        fixed = max(1, used // 4)
        moved = fixed + (places - fixed + rotation * (used - fixed)) % max(1, number_of - fixed)
        return jnp.zeros((number_of,), jnp.int32).at[sequence[jnp.where(places < fixed, places, moved)]].set(jnp.asarray(tallies, jnp.int32))

    tallies = jnp.where(number % 4 == 0, named(heavy_load, number // 4), named(common, number - number // 4 - 1))
    mixed = jax.random.permutation(jax.random.fold_in(own, 3), number_of)
    source_of, taker = mixed[0:number_of // 2 * 2:2], mixed[1:number_of // 2 * 2:2]
    room = jnp.minimum(tallies[source_of] - 1, most - tallies[taker]) // 2
    room = jnp.where((source_of == sequence[0]) | (taker == sequence[0]) | (tallies[taker] == 0), 0, jnp.maximum(room, 0))
    moved = jax.random.randint(jax.random.fold_in(own, 4), (number_of // 2,), 0, 1 << 20) % (room + 1)
    tallies = tallies.at[source_of].add(-moved).at[taker].add(moved)
    items = jnp.searchsorted(jnp.cumsum(tallies), jnp.arange(rows * top), side="right").astype(jnp.int32)
    table = items.reshape(top, rows).T
    table = table[jax.random.permutation(jax.random.fold_in(own, 1), rows)]
    rotation = jax.random.randint(jax.random.fold_in(own, 2), (rows, 1), 0, top)
    return jnp.take_along_axis(table, (jnp.arange(top)[None, :] + rotation) % top, axis=1)


def portions_of(number_of, total, most, skew, full):
    portions = [(1 << 20) // math.isqrt(rank ** skew) + 1 for rank in range(1, number_of + 1)]
    largest = most if full else min(most, max(-(-total // number_of), total * portions[0] // sum(portions)))
    least = 1 if total - largest >= number_of - 1 else 0
    given, rest = [largest] + [least] * (number_of - 1), total - largest - least * (number_of - 1)
    while rest > 0:
        free = [i for i in range(1, number_of) if given[i] < largest] or [i for i in range(1, number_of) if given[i] < most]
        pool, budget = sum([portions[i] for i in free]), rest
        for i in free:
            addition = min(most - given[i], max(1, budget * portions[i] // pool), rest)
            given[i] = given[i] + addition
            rest = rest - addition
    return np.array(given)


def centred(key, dims, scale, limit, split=(), held_as=jnp.bfloat16):
    drawn = jax.random.normal(key, dims, jnp.float32) * scale
    if len(split) > 0:
        drawn = shard_levels(key, dims, split, -0.22, 0.18) * drawn
    return jnp.clip(drawn, min=-limit, max=limit).astype(held_as)


def setup_inputs(seed: int = 0) -> dict:
    arg_keys = jax.random.split(jax.random.key(seed), 18)
    cell_query_heads = centred(arg_keys[0], (SEQ, CELL_HEADS * HD), 1.0, 6.0, ((0, 8), (1, 4)))
    cell_key_heads = centred(arg_keys[1], (SEQ, CELL_HEADS * HD), 1.0, 6.0, ((0, 8), (1, 4)))
    cell_value_heads = centred(arg_keys[2], (SEQ, CELL_HEADS * HD), 1.0, 6.0, ((0, 8), (1, 4)))
    output_gate_logits = centred(arg_keys[3], (SEQ, CELL_HEADS * HD), 1.0, 6.0, ((0, 8), (1, 4)))
    input_gate_log = draw_input_gate_log(jax.random.fold_in(arg_keys[17], 71), 0)
    forget_gate_logits = draw_forget_gate_logits(jax.random.fold_in(arg_keys[17], 71), 0)
    extra_log_decay = draw_extra_log_decay(jax.random.fold_in(arg_keys[17], 71), 0)
    documents = jnp.searchsorted(jnp.cumsum(ragged(arg_keys[7], DOCS, SEQ, DOC_MOST, 1)), jnp.arange(SEQ), side="right").astype(jnp.int32)
    head_norm_gain = jnp.clip(1.0 + 0.18 * jax.random.normal(arg_keys[8], (CELL_HEADS * HD,), jnp.float32), 0.1, 1.9)
    stream = centred(arg_keys[9], (SEQ, D), 1.0, 6.0, ((0, 8), (1, 4)))
    output_weight = centred(arg_keys[10], (CELL_HEADS * HD, D), (CELL_HEADS * HD) ** -0.5, 0.125, ((1, 4),))
    expert_norm_gain = jnp.clip(1.0 + 0.18 * jax.random.normal(arg_keys[11], (D,), jnp.float32), 0.099609375, 1.8984375).astype(jnp.bfloat16)
    expert_choice_index_keys = jax.random.split(jax.random.fold_in(arg_keys[12], 1), SEQ // TOKENS_PER_SHARD)
    expert_choice_index_turns = jax.random.permutation(jax.random.fold_in(arg_keys[12], 3), SEQ // TOKENS_PER_SHARD)
    expert_choice_index = jax.vmap(lambda own, number: assign_block(jax.random.fold_in(arg_keys[12], 2), own, number, TOKENS_PER_SHARD, EXPERTS, TOPK, CAP, 2))(expert_choice_index_keys, expert_choice_index_turns).reshape((SEQ, TOPK))
    routing_weight = jnp.clip(0.2 + 0.8 * jax.random.uniform(arg_keys[13], (SEQ, TOPK), jnp.float32) ** shard_levels(arg_keys[13], (SEQ, TOPK), ((0, 8),), -0.2, 0.2), 0.2, 1.0)
    gate_weight = centred(arg_keys[14], (EXPERTS, D, FF), D ** -0.5, 0.09375, ((0, 8), (2, 4)))
    up_weight = centred(arg_keys[15], (EXPERTS, D, FF), D ** -0.5, 0.09375, ((0, 8), (2, 4)))
    down_weight = centred(arg_keys[16], (EXPERTS, FF, D), FF ** -0.5, 0.125, ((0, 8), (2, 4)))
    return dict(cell_query_heads=cell_query_heads, cell_key_heads=cell_key_heads, cell_value_heads=cell_value_heads, output_gate_logits=output_gate_logits, input_gate_log=input_gate_log, forget_gate_logits=forget_gate_logits, extra_log_decay=extra_log_decay, documents=documents, head_norm_gain=head_norm_gain, stream=stream, output_weight=output_weight, expert_norm_gain=expert_norm_gain, expert_choice_index=expert_choice_index, routing_weight=routing_weight, gate_weight=gate_weight, up_weight=up_weight, down_weight=down_weight)


EPSILON = 1e-06
LOW_LOG = -1e+30
HIGHEST = lax.Precision.HIGHEST

def empty_summary(heads, width):
    return (jnp.zeros((heads, width, width), jnp.float32), jnp.zeros((heads, width), jnp.float32), jnp.full((heads,), LOW_LOG, jnp.float32), jnp.zeros((heads,), jnp.float32), jnp.zeros((), jnp.int32), jnp.full((), -1, jnp.int32), jnp.full((), -1, jnp.int32))

def block_summary(key_f, value_f, decay_logarithm, input_gate_log, documents, first_global):
    length = documents.shape[0]
    positions = jnp.arange(length, dtype=jnp.int32)
    cumulative = jnp.cumsum(decay_logarithm, axis=0)
    total_log = cumulative[-1]
    prior_log = cumulative - decay_logarithm
    starts = jnp.concatenate([jnp.reshape(first_global, (1,)), documents[1:] != documents[:-1]])
    inside = jnp.any(starts)
    last_start = jnp.max(jnp.where(starts, positions, -1))
    base_log = lax.optimization_barrier(jnp.sum(jnp.where((positions == last_start)[:, None], prior_log, 0.0), axis=0))
    in_last = (documents == documents[-1])[:, None]
    weight_log = total_log[None, :] - cumulative + input_gate_log
    peak_log = lax.optimization_barrier(jnp.max(jnp.where(in_last, weight_log, LOW_LOG), axis=0))
    peak_log = jnp.where(inside, jnp.maximum(peak_log, total_log - base_log), peak_log)
    weights = jnp.where(in_last, jnp.exp(jnp.minimum(weight_log - peak_log[None, :], 0.0)), 0.0)
    matrix = jnp.einsum('lhd,lhe->hde', weights[:, :, None] * key_f, value_f, precision=HIGHEST)
    normer = lax.optimization_barrier(jnp.sum(weights[:, :, None] * key_f, axis=0))
    return (matrix, normer, peak_log, total_log, inside.astype(jnp.int32), documents[0], documents[-1])

def combine(early, late):
    broken = late[5] != early[6]
    carry_matrix = jnp.where(broken, 0.0, early[0])
    carry_normer = jnp.where(broken, 0.0, early[1])
    carry_peak = jnp.where(broken, 0.0, early[2])
    joined = jnp.maximum(late[3] + carry_peak, late[2])
    older = jnp.exp(late[3] + carry_peak - joined)
    newer = jnp.exp(late[2] - joined)
    resets = late[4] > 0
    matrix = jnp.where(resets, late[0], older[:, None, None] * carry_matrix + newer[:, None, None] * late[0])
    normer = jnp.where(resets, late[1], older[:, None] * carry_normer + newer[:, None] * late[1])
    peak_log = jnp.where(resets, late[2], joined)
    flags = jnp.maximum(jnp.maximum(early[4], late[4]), broken.astype(jnp.int32))
    merged = (matrix, normer, peak_log, early[3] + late[3], flags, early[5], late[6])
    early_empty = early[6] < 0
    late_empty = late[6] < 0
    return tuple((jnp.where(early_empty, second, jnp.where(late_empty, first_item, joint)) for first_item, second, joint in zip(early, late, merged)))

def block_output(query_f, key_f, value_f, decay_logarithm, input_gate_log, documents, prefix):
    prev_matrix, prev_normer, prev_peak, _, _, _, prev_last = prefix
    length = documents.shape[0]
    positions = jnp.arange(length, dtype=jnp.int32)
    cumulative = jnp.cumsum(decay_logarithm, axis=0)
    prior_log = cumulative - decay_logarithm
    before = jnp.concatenate([jnp.reshape(prev_last, (1,)), documents[:-1]])
    starts = documents != before
    last_start = lax.cummax(jnp.where(starts, positions, -1), axis=0)
    started = last_start >= 0
    picker = (positions[None, :] == last_start[:, None]).astype(jnp.float32)
    base_log = jnp.dot(picker, prior_log, precision=HIGHEST)
    carry_log = (cumulative + jnp.where(started[:, None], -base_log, prev_peak[None, :])).T
    same_doc = (documents[:, None] == documents[None, :]) & (positions[:, None] >= positions[None, :])
    cum_heads = cumulative.T
    pair_log = cum_heads[:, :, None] - cum_heads[:, None, :] + input_gate_log.T[:, None, :]
    pair_log = jnp.where(same_doc[None], pair_log, LOW_LOG)
    peak_log = jnp.maximum(carry_log, lax.optimization_barrier(jnp.max(pair_log, axis=-1)))
    weights = jnp.exp(pair_log - peak_log[:, :, None])
    scores = jnp.einsum('lhd,shd->hls', query_f, key_f, precision=HIGHEST) * weights
    carry_scale = jnp.where(started[None, :], 0.0, jnp.exp(carry_log - peak_log))
    numer = jnp.einsum('hls,she->hle', scores, value_f, precision=HIGHEST)
    numer = numer + carry_scale[:, :, None] * jnp.einsum('lhd,hde->hle', query_f, prev_matrix, precision=HIGHEST)
    denom = lax.optimization_barrier(jnp.sum(scores, axis=-1)) + carry_scale * jnp.einsum('lhd,hd->hl', query_f, prev_normer, precision=HIGHEST)
    cell_vals = numer / jnp.maximum(jnp.abs(denom), jnp.exp(-peak_log))[:, :, None]
    return jnp.transpose(cell_vals, (1, 0, 2))

def finish_cell(cell_vals, output_gate_logits, head_norm_gain):
    length, heads, width = cell_vals.shape
    gated_cell = jax.nn.sigmoid(output_gate_logits.astype(jnp.float32)).reshape(length, heads, width) * cell_vals
    scaled = gated_cell * lax.rsqrt(lax.optimization_barrier(jnp.mean(gated_cell * gated_cell, axis=-1, keepdims=True)) + EPSILON)
    scaled = scaled * head_norm_gain.astype(jnp.float32).reshape(heads, width)
    return scaled.reshape(length, heads * width).astype(jnp.bfloat16)

def memory_cell_layer(cell_query_heads, cell_key_heads, cell_value_heads, output_gate_logits, input_gate_log, forget_gate_logits, extra_log_decay, documents, head_norm_gain):
    seq_len = documents.shape[0]
    block_list = seq_len // TOKENS_PER_SHARD
    shaped = (block_list, TOKENS_PER_SHARD, CELL_HEADS, HD)
    query_f = cell_query_heads.astype(jnp.float32).reshape(shaped)
    key_f = cell_key_heads.astype(jnp.float32).reshape(shaped) * HD ** (-0.5)
    value_f = cell_value_heads.astype(jnp.float32).reshape(shaped)
    decay_logarithm = (jax.nn.log_sigmoid(forget_gate_logits) + extra_log_decay).reshape(block_list, TOKENS_PER_SHARD, CELL_HEADS)
    gates = input_gate_log.reshape(block_list, TOKENS_PER_SHARD, CELL_HEADS)
    docs = documents.reshape(block_list, TOKENS_PER_SHARD)
    firsts = jnp.arange(block_list, dtype=jnp.int32) == 0
    summaries = lax.map(lambda items: block_summary(*items), (key_f, value_f, decay_logarithm, gates, docs, firsts))

    def advance(running, summary):
        return (combine(running, summary), running)
    _, prefixes = lax.scan(advance, empty_summary(CELL_HEADS, HD), summaries)
    cell_vals = lax.map(lambda items: block_output(*items), (query_f, key_f, value_f, decay_logarithm, gates, docs, prefixes))
    return finish_cell(cell_vals.reshape(seq_len, CELL_HEADS, HD), output_gate_logits, head_norm_gain)

def experts_layer(normed, expert_choice_index, routing_weight, gate_weight, up_weight, down_weight):
    seq_len = normed.shape[0]
    block_list = seq_len // TOKENS_PER_SHARD
    grouped = expert_choice_index.reshape(block_list, TOKENS_PER_SHARD * TOPK)
    onehot = (grouped[:, :, None] == jnp.arange(EXPERTS, dtype=jnp.int32)[None, None, :]).astype(jnp.int32)
    rank_in = lax.optimization_barrier(jnp.sum((jnp.cumsum(onehot, axis=1) - onehot) * onehot, axis=2))
    block_of = jnp.arange(block_list, dtype=jnp.int32)[:, None]
    slot_of = (grouped * (N_SP * CAP) + block_of * CAP + rank_in).reshape(-1).astype(jnp.int32)
    sources = jnp.repeat(normed, TOPK, axis=0)
    buffer = jnp.zeros((EXPERTS * N_SP * CAP, D), jnp.bfloat16).at[slot_of].set(sources)

    def run_expert(operands):
        row_block, gate_e, up_e, down_e = operands
        gate_act = jnp.dot(row_block, gate_e, preferred_element_type=jnp.float32)
        upward = jnp.dot(row_block, up_e, preferred_element_type=jnp.float32)
        hidden = (jax.nn.silu(gate_act) * upward).astype(jnp.bfloat16)
        return jnp.dot(hidden, down_e, preferred_element_type=jnp.float32).astype(jnp.bfloat16)
    served = lax.map(run_expert, (buffer.reshape(EXPERTS, N_SP * CAP, D), gate_weight, up_weight, down_weight))
    picked = served.reshape(-1, D)[slot_of].astype(jnp.float32).reshape(seq_len, TOPK, D)
    return lax.optimization_barrier(jnp.sum(picked * routing_weight[:, :, None], axis=1))

def reference(cell_query_heads, cell_key_heads, cell_value_heads, output_gate_logits, input_gate_log, forget_gate_logits, extra_log_decay, documents, head_norm_gain, stream, output_weight, expert_norm_gain, expert_choice_index, routing_weight, gate_weight, up_weight, down_weight):
    memory_cell_output = memory_cell_layer(cell_query_heads, cell_key_heads, cell_value_heads, output_gate_logits, input_gate_log, forget_gate_logits, extra_log_decay, documents, head_norm_gain)
    resid = (stream.astype(jnp.float32) + jnp.dot(memory_cell_output, output_weight, preferred_element_type=jnp.float32)).astype(jnp.bfloat16)
    rows_f = resid.astype(jnp.float32)
    normed = rows_f * lax.rsqrt(lax.optimization_barrier(jnp.mean(rows_f * rows_f, axis=1, keepdims=True)) + EPSILON)
    normed = (normed * expert_norm_gain.astype(jnp.float32)[None, :]).astype(jnp.bfloat16)
    mixed = experts_layer(normed, expert_choice_index, routing_weight, gate_weight, up_weight, down_weight)
    return (rows_f + mixed).astype(jnp.bfloat16)
```

```python
import functools

import jax
import jax.numpy as jnp
from jax import lax
from jax.experimental import pallas as pl
from jax.experimental.pallas import tpu as pltpu
from jax.sharding import PartitionSpec as P

HD = 128
TOPK = 2
EPSILON = 1e-06
LOW_LOG = -1e30
HIGHEST = lax.Precision.HIGHEST
MESH = pl.DeviceIdType.MESH
VMEM_LIMIT = 60 * 1024 * 1024
SUB = 8
EACH = 2
f32, bf16 = jnp.float32, jnp.bfloat16


def remote(src, dst, send, recv, where):
    return pltpu.make_async_remote_copy(src, dst, send, recv, device_id=where, device_id_type=MESH)


def near_peers(teams, j):
    if teams == 4:
        return [j + 1 - 2 * lax.rem(j, 2), lax.rem(j + 2, 4)]
    return [lax.rem(j + step, teams) for step in range(1, teams)]


def all_peers(teams, j):
    if teams == 4:
        return near_peers(teams, j) + [3 - j]
    return near_peers(teams, j)


def spread_own(teams, j, buf, row, height, width, chunk, send, recv):
    view = buf.at[pl.ds(row, height), pl.ds(pl.multiple_of(j * width, 128), width)]
    return [
        remote(view, view, send.at[chunk, turn], recv.at[chunk, turn], {"tp": peer})
        for turn, peer in enumerate(near_peers(teams, j))
    ]


def spread_relay(teams, j, buf, row, height, width, chunk, send, recv):
    if teams != 4:
        return []
    half = height // 2
    across, along = near_peers(teams, j)
    first = buf.at[pl.ds(row, half), pl.ds(pl.multiple_of(across * width, 128), width)]
    second = buf.at[pl.ds(row + half, half), pl.ds(pl.multiple_of(along * width, 128), width)]
    return [
        remote(first, first, send.at[chunk, 2], recv.at[chunk, 2], {"tp": along}),
        remote(second, second, send.at[chunk, 3], recv.at[chunk, 3], {"tp": across}),
    ]


def nt(a, b, precision=None):
    return lax.dot_general(
        a, b, (((1,), (1,)), ((), ())), precision=precision, preferred_element_type=f32
    )


def kernel(
    groups, teams, heads, reach, cap, each, chunks,
    query, key, value, gate_out, table, head_gain, stream, row_gain, wo_hbm, gate_hbm, up_hbm, down_hbm,
    out,
    kbuf, vbuf, tbuf, cell, ssq, chooser, comb, resid, normed, packed, rows, hidden, result, returned,
    wo, gate, up, down,
    load_sem, k_send, k_recv, v_send, v_recv, m_send, m_recv, c_send, c_recv, s_send, s_recv,
    z_send, z_recv, t_send, t_recv, h_send, h_recv, r_send, r_recv,
):
    g, j = lax.axis_index("sp"), lax.axis_index("tp")
    tokens, width = stream.shape
    hide = gate.shape[1]
    span = heads * HD
    slots = groups * cap
    tall = each * cap
    model = width * teams
    loads = [
        pltpu.make_async_copy(wo_hbm, wo, load_sem.at[0]),
        pltpu.make_async_copy(gate_hbm.at[0], gate, load_sem.at[1]),
        pltpu.make_async_copy(up_hbm.at[0], up, load_sem.at[2]),
        pltpu.make_async_copy(down_hbm.at[0], down, load_sem.at[3]),
    ]
    for load in loads:
        load.start()
    barrier = pltpu.get_barrier_semaphore()
    for step in range(1, groups):
        pl.semaphore_signal(
            barrier, inc=1, device_id={"sp": lax.rem(g + step, groups)}, device_id_type=MESH
        )
    peers = all_peers(teams, j)
    for peer in peers:
        pl.semaphore_signal(barrier, inc=1, device_id={"tp": peer}, device_id_type=MESH)
    pl.semaphore_wait(barrier, groups - 1 + len(peers))

    def send_table(r):
        return remote(table, tbuf.at[r - 1], m_send.at[r - 1], m_recv.at[r - 1], {"sp": g + r})

    def send_pair(r, h):
        cols = pl.ds(h * HD, HD)
        return [
            remote(key.at[:, cols], kbuf.at[r - 1, :, cols], k_send.at[r - 1, h], k_recv.at[r - 1, h], {"sp": g + r}),
            remote(value.at[:, cols], vbuf.at[r - 1, :, cols], v_send.at[r - 1, h], v_recv.at[r - 1, h], {"sp": g + r}),
        ]

    for r in range(1, reach + 1):

        @pl.when(g + r < groups)
        def _(r=r):
            send_table(r).start()

    for h in range(heads):
        for r in range(1, reach + 1):

            @pl.when(g + r < groups)
            def _(r=r, h=h):
                for copy in send_pair(r, h):
                    copy.start()

    for r in range(1, reach + 1):

        @pl.when(g < r)
        def _(r=r):
            kbuf[r - 1] = jnp.zeros_like(kbuf[r - 1])
            vbuf[r - 1] = jnp.zeros_like(vbuf[r - 1])
            tbuf[r - 1] = jnp.full(tbuf.shape[1:], -1.0, f32)

    down_iota = lax.broadcasted_iota(jnp.int32, (tokens, tokens), 0)
    across_iota = lax.broadcasted_iota(jnp.int32, (tokens, tokens), 1)
    causal = across_iota <= down_iota
    lower = causal.astype(f32)
    upper = (down_iota <= across_iota).astype(f32)
    strict = (down_iota < across_iota).astype(bf16)
    eye = (down_iota == across_iota).astype(f32)
    misc = table[2 * SUB : 3 * SUB, :]
    columns = nt(eye, misc, HIGHEST)
    expert_pad = -(-groups // SUB) * SUB
    expert_iota = lax.broadcasted_iota(jnp.int32, (expert_pad, tokens), 0).astype(f32)
    member = jnp.zeros((expert_pad, tokens), f32)
    weighted = jnp.zeros((expert_pad, tokens), f32)
    for ordinal in range(TOPK):
        chosen = expert_iota == misc[1 + ordinal : 2 + ordinal, :]
        member = member + jnp.where(chosen, 1.0, 0.0)
        weighted = weighted + jnp.where(
            chosen, misc[1 + TOPK + ordinal : 2 + TOPK + ordinal, :], 0.0
        )
    rank = jnp.dot(member.astype(bf16), strict, preferred_element_type=f32)
    rank = jnp.where(member > 0.5, rank, -1.0)
    cap_iota = lax.broadcasted_iota(jnp.int32, (cap, tokens), 0).astype(f32)
    for e in range(groups):
        chooser[e * cap : (e + 1) * cap, :] = jnp.where(
            cap_iota == rank[e : e + 1, :], 1.0, 0.0
        ).astype(bf16)
    slot_line = lax.broadcasted_iota(jnp.int32, (1, slots), 1).astype(f32)
    expert_line = jnp.floor((slot_line + 0.5) * (1.0 / cap))
    place_line = slot_line - expert_line * cap
    expand = (
        lax.broadcasted_iota(jnp.int32, (expert_pad, slots), 0).astype(f32) == expert_line
    ).astype(f32)
    rank_wide = jnp.dot(nt(eye, rank), expand, preferred_element_type=f32)
    weight_wide = jnp.dot(
        nt(eye, weighted, HIGHEST), expand, precision=HIGHEST, preferred_element_type=f32
    )
    comb[...] = jnp.where(rank_wide == place_line, weight_wide, 0.0).astype(bf16)

    decay = table[0:SUB, :]
    entry = table[SUB : 2 * SUB, :]
    doc_col = columns[:, 0:1]
    own_mask = causal & (doc_col == misc[0:1, :])
    cum_col = nt(lower, decay, HIGHEST)
    cum_row = jnp.dot(decay, upper, precision=HIGHEST, preferred_element_type=f32)
    carry = nt(own_mask.astype(f32), decay, HIGHEST)
    masks, terms = [own_mask], [entry - cum_row]

    for r in range(1, reach + 1):

        @pl.when(g >= r)
        def _(r=r):
            send_table(r).wait_recv()

    behind = jnp.zeros((SUB, 1), f32)
    for r in range(1, reach + 1):
        decay_r = tbuf[r - 1, 0:SUB, :]
        mask_r = doc_col == tbuf[r - 1, 2 * SUB : 2 * SUB + 1, :]
        cum_r = jnp.dot(decay_r, upper, precision=HIGHEST, preferred_element_type=f32)
        total_r = cum_r[:, tokens - 1 : tokens]
        terms.append(tbuf[r - 1, SUB : 2 * SUB, :] + ((total_r - cum_r) + behind))
        behind = behind + total_r
        carry = carry + nt(mask_r.astype(f32), decay_r, HIGHEST)
        masks.append(mask_r)

    def cell_copies(h):
        view = cell.at[:, pl.ds(pl.multiple_of(j * span + h * HD, 128), HD)]
        return [
            remote(view, view, c_send.at[h, turn], c_recv.at[h, turn], {"tp": peer})
            for turn, peer in enumerate(peers)
        ]

    for h in range(heads):
        cols = slice(h * HD, (h + 1) * HD)
        for r in range(1, reach + 1):

            @pl.when(g >= r)
            def _(r=r, h=h):
                for copy in send_pair(r, h):
                    copy.wait_recv()

        q_h = query[:, cols]
        keys = [key[:, cols]] + [kbuf[r, :, cols] for r in range(reach)]
        values = [value[:, cols]] + [vbuf[r, :, cols] for r in range(reach)]
        peak = carry[:, h : h + 1]
        logs = []
        for mask, term in zip(masks, terms):
            log = jnp.where(mask, cum_col[:, h : h + 1] + term[h : h + 1, :], LOW_LOG)
            peak = jnp.maximum(peak, jnp.max(log, axis=1, keepdims=True))
            logs.append(log)
        denom = jnp.zeros((tokens, 1), f32)
        numer = jnp.zeros((tokens, HD), f32)
        for log, k_b, v_b in zip(logs, keys, values):
            score = nt(q_h, k_b) * (HD ** -0.5) * jnp.exp(log - peak)
            denom = denom + jnp.sum(score, axis=1, keepdims=True)
            numer = numer + jnp.dot(score.astype(bf16), v_b, preferred_element_type=f32)
        value_h = numer / jnp.maximum(jnp.abs(denom), jnp.exp(-peak))
        value_h = value_h * jax.nn.sigmoid(gate_out[:, cols].astype(f32))
        square = jnp.sum(value_h * value_h, axis=1, keepdims=True) * (1.0 / HD)
        value_h = value_h * lax.rsqrt(square + EPSILON) * head_gain[:, cols]
        cell[:, pl.ds(pl.multiple_of(j * span + h * HD, 128), HD)] = value_h.astype(bf16)
        for copy in cell_copies(h):
            copy.start()

    loads[0].wait()
    half = max(1, heads // 2)
    projected = stream[...].astype(f32)
    for first in range(0, heads, half):
        for h in range(first, first + half):
            for copy in cell_copies(h):
                copy.wait_recv()
        for p in range(teams):
            piece = slice(p * span + first * HD, p * span + (first + half) * HD)
            projected = projected + jnp.dot(cell[:, piece], wo[piece, :], preferred_element_type=f32)
    resid[...] = projected.astype(bf16)
    rows_f = resid[...].astype(f32)
    squares = jnp.sum(rows_f * rows_f, axis=1, keepdims=True)
    ssq[j] = jnp.broadcast_to(squares, (tokens, tokens)).T[0:SUB, :]

    def square_copies():
        return [
            remote(ssq.at[j], ssq.at[j], s_send.at[turn], s_recv.at[turn], {"tp": peer})
            for turn, peer in enumerate(peers)
        ]

    for copy in square_copies():
        copy.start()
    for copy in square_copies():
        copy.wait_recv()
    total = ssq[0]
    for p in range(1, teams):
        total = total + ssq[p]
    total = jnp.broadcast_to(total[0:1, :], (tokens, tokens)).T[:, 0:1]
    scale = lax.rsqrt(total * (1.0 / model) + EPSILON)
    normed[...] = (rows_f * scale * row_gain[...].astype(f32)).astype(bf16)

    own = pl.ds(pl.multiple_of(g * cap, cap), cap)
    mine = pl.ds(pl.multiple_of(j * width, 128), width)
    block = g // each

    def chunk_of(k):
        if chunks == 4:
            pair = block + 1 - 2 * lax.rem(block, 2)
            return jnp.where(
                k == 0, block, jnp.where(k == 1, lax.rem(block + 2, 4), jnp.where(k == 2, 3 - block, pair))
            )
        return lax.rem(block + k, chunks)

    def slot_rows(e):
        return pl.ds(pl.multiple_of(e * cap, cap), cap)

    def dispatch(target):
        return remote(
            packed.at[slot_rows(target)], rows.at[own, mine], z_send.at[target], z_recv.at[g], {"sp": target}
        )

    def give_back(target):
        return remote(
            result.at[slot_rows(target)], returned.at[own], r_send.at[target], r_recv.at[g], {"sp": target}
        )

    def over_others(body):
        def one(k, carry_):
            c = chunk_of(k)
            for p in range(each):
                target = c * each + p

                @pl.when(target != g)
                def _():
                    body(target)

            return carry_

        lax.fori_loop(0, chunks, one, 0)

    def pack(k, carry_):
        c = chunk_of(k)
        at = pl.ds(pl.multiple_of(c * tall, tall), tall)
        packed[at, :] = jnp.dot(chooser[at, :], normed[...], preferred_element_type=f32).astype(bf16)

        @pl.when(k == 0)
        def _():
            rows[own, mine] = packed[own, :]

        for p in range(each):
            target = c * each + p

            @pl.when(target != g)
            def _():
                dispatch(target).start()

        return carry_

    lax.fori_loop(0, chunks, pack, 0)

    def row_of(c):
        return pl.multiple_of(c * tall, tall)

    def start_spread(c):
        for p in range(each):
            source = c * each + p

            @pl.when(source != g)
            def _():
                place = rows.at[slot_rows(source), mine]
                remote(place, place, z_send.at[source], z_recv.at[source], {"sp": source}).wait_recv()

        for copy in spread_own(teams, j, rows, row_of(c), tall, width, c, t_send, t_recv):
            copy.start()

    def finish(c):
        row = row_of(c)
        for copy in spread_relay(teams, j, hidden, row, tall, hide, c, h_send, h_recv):
            copy.wait_recv()
        result[pl.ds(row, tall), :] = jnp.dot(
            hidden[pl.ds(row, tall), :], down[...], preferred_element_type=f32
        ).astype(bf16)
        for p in range(each):
            target = c * each + p

            @pl.when(target != g)
            def _():
                give_back(target).start()

            @pl.when(target == g)
            def _():
                returned[own, :] = result[own, :]

    def hidden_relay(c):
        row = row_of(c)
        for copy in spread_own(teams, j, hidden, row, tall, hide, c, h_send, h_recv):
            copy.wait_recv()
        for copy in spread_relay(teams, j, hidden, row, tall, hide, c, h_send, h_recv):
            copy.start()

    start_spread(chunk_of(0))
    for load in loads[1:]:
        load.wait()

    def stage(k, carry_):
        c = chunk_of(k)
        last = chunk_of(jnp.maximum(k - 1, 0))
        row = row_of(c)

        @pl.when(k < chunks)
        def _():
            for copy in spread_own(teams, j, rows, row, tall, width, c, t_send, t_recv):
                copy.wait_recv()
            for copy in spread_relay(teams, j, rows, row, tall, width, c, t_send, t_recv):
                copy.start()

        @pl.when(k < chunks - 1)
        def _():
            start_spread(chunk_of(k + 1))

        @pl.when(k >= 1)
        def _():
            hidden_relay(last)

        @pl.when(k < chunks)
        def _():
            for copy in spread_relay(teams, j, rows, row, tall, width, c, t_send, t_recv):
                copy.wait_recv()
            block_rows = rows[pl.ds(row, tall), :]
            opened = jnp.dot(block_rows, gate[...], preferred_element_type=f32)
            raised = jnp.dot(block_rows, up[...], preferred_element_type=f32)
            made = (opened * jax.nn.sigmoid(opened) * raised).astype(bf16)
            hidden[pl.ds(row, tall), pl.ds(pl.multiple_of(j * hide, 128), hide)] = made
            for copy in spread_own(teams, j, hidden, row, tall, hide, c, h_send, h_recv):
                copy.start()

        @pl.when(k >= 1)
        def _():
            finish(last)

        return carry_

    lax.fori_loop(0, chunks + 1, stage, 0)

    def await_back(source):
        place = returned.at[slot_rows(source)]
        remote(place, place, r_send.at[source], r_recv.at[source], {"sp": source}).wait_recv()

    over_others(await_back)
    mixed = jnp.dot(comb[...], returned[...], preferred_element_type=f32)
    out[...] = (resid[...].astype(f32) + mixed).astype(bf16)

    for r in range(1, reach + 1):

        @pl.when(g + r < groups)
        def _(r=r):
            send_table(r).wait_send()
            for h in range(heads):
                for copy in send_pair(r, h):
                    copy.wait_send()

    for h in range(heads):
        for copy in cell_copies(h):
            copy.wait_send()
    for copy in square_copies():
        copy.wait_send()
    over_others(lambda target: dispatch(target).wait_send())
    over_others(lambda target: give_back(target).wait_send())

    def drain(c, carry_):
        row = row_of(c)
        for spread in (spread_own, spread_relay):
            for copy in spread(teams, j, rows, row, tall, width, c, t_send, t_recv):
                copy.wait_send()
            for copy in spread(teams, j, hidden, row, tall, hide, c, h_send, h_recv):
                copy.wait_send()
        return carry_

    lax.fori_loop(0, chunks, drain, 0)


def padded(a):
    return jnp.pad(a, ((0, SUB - a.shape[0]), (0, 0)))


def per_device(
    cell_query_heads,
    cell_key_heads,
    cell_value_heads,
    output_gate_logits,
    input_gate_log,
    forget_gate_logits,
    extra_log_decay,
    documents,
    head_norm_gain,
    stream,
    output_weight,
    expert_norm_gain,
    expert_choice_index,
    routing_weight,
    gate_weight,
    up_weight,
    down_weight,
):
    groups, teams = lax.axis_size("sp"), lax.axis_size("tp")
    tokens, heads = input_gate_log.shape
    span = heads * HD
    width = stream.shape[1]
    _, model, hide = gate_weight.shape
    _, hidden_all, _ = down_weight.shape
    experts_all = groups * gate_weight.shape[0]
    cap = 2 * tokens * TOPK // experts_all
    slots = groups * cap
    each = max(1, min(groups, EACH * 64 // cap))
    chunks = groups // each
    reach = max(1, groups // 4)
    ways = max(4, teams)
    others = teams - 1
    decay = jax.nn.log_sigmoid(forget_gate_logits) + extra_log_decay
    misc = jnp.concatenate(
        [documents.astype(f32)[None, :], expert_choice_index.astype(f32).T, routing_weight.T], axis=0
    )
    table = jnp.concatenate([padded(decay.T), padded(input_gate_log.T), padded(misc)], axis=0)
    vmem = pl.BlockSpec(memory_space=pltpu.VMEM)
    hbm = pl.BlockSpec(memory_space=pl.ANY)
    dma = pltpu.SemaphoreType.DMA
    return pl.pallas_call(
        functools.partial(kernel, groups, teams, heads, reach, cap, each, chunks),
        out_shape=jax.ShapeDtypeStruct((tokens, width), bf16),
        in_specs=[vmem] * 8 + [hbm] * 4,
        out_specs=vmem,
        scratch_shapes=[
            pltpu.VMEM((reach, tokens, span), bf16),
            pltpu.VMEM((reach, tokens, span), bf16),
            pltpu.VMEM((reach, 3 * SUB, tokens), f32),
            pltpu.VMEM((tokens, teams * span), bf16),
            pltpu.VMEM((teams, SUB, tokens), f32),
            pltpu.VMEM((slots, tokens), bf16),
            pltpu.VMEM((tokens, slots), bf16),
            pltpu.VMEM((tokens, width), bf16),
            pltpu.VMEM((tokens, width), bf16),
            pltpu.VMEM((slots, width), bf16),
            pltpu.VMEM((slots, model), bf16),
            pltpu.VMEM((slots, hidden_all), bf16),
            pltpu.VMEM((slots, width), bf16),
            pltpu.VMEM((slots, width), bf16),
            pltpu.VMEM(output_weight.shape, bf16),
            pltpu.VMEM((model, hide), bf16),
            pltpu.VMEM((model, hide), bf16),
            pltpu.VMEM((hidden_all, width), bf16),
            dma((4,)),
            dma((reach, heads)),
            dma((reach, heads)),
            dma((reach, heads)),
            dma((reach, heads)),
            dma((reach,)),
            dma((reach,)),
            dma((heads, others)),
            dma((heads, others)),
            dma((others,)),
            dma((others,)),
            dma((groups,)),
            dma((groups,)),
            dma((chunks, ways)),
            dma((chunks, ways)),
            dma((chunks, ways)),
            dma((chunks, ways)),
            dma((groups,)),
            dma((groups,)),
        ],
        compiler_params=pltpu.CompilerParams(
            collective_id=1, has_side_effects=True, vmem_limit_bytes=VMEM_LIMIT
        ),
    )(
        cell_query_heads,
        cell_key_heads,
        cell_value_heads,
        output_gate_logits,
        table,
        head_norm_gain[None, :],
        stream,
        expert_norm_gain[None, :],
        output_weight,
        gate_weight,
        up_weight,
        down_weight,
    )


def solution(mesh):
    placed = (
        P("sp", "tp"),
        P("sp", "tp"),
        P("sp", "tp"),
        P("sp", "tp"),
        P("sp", "tp"),
        P("sp", "tp"),
        P("sp", "tp"),
        P("sp"),
        P("tp"),
        P("sp", "tp"),
        P(None, "tp"),
        P("tp"),
        P("sp", None),
        P("sp", None),
        P("sp", None, "tp"),
        P("sp", None, "tp"),
        P("sp", None, "tp"),
    )
    return jax.shard_map(
        per_device, mesh=mesh, in_specs=placed, out_specs=P("sp", "tp"), check_vma=False
    )
```

```python
import functools

import jax
import jax.numpy as jnp
from jax import lax
from jax.experimental import pallas as pl
from jax.experimental.pallas import tpu as pltpu
from jax.sharding import PartitionSpec as P

HD = 128
TOPK = 2
EPSILON = 1e-06
LOW_LOG = -1e30
HIGHEST = lax.Precision.HIGHEST
MESH = pl.DeviceIdType.MESH
VMEM_LIMIT = 60 * 1024 * 1024
SUB = 8
EACH = 1
ORDER = ((0, 0), (1, 0), (2, 0), (2, 1), (3, 0), (3, 1), (1, 1), (0, 1))
f32, bf16 = jnp.float32, jnp.bfloat16


def remote(src, dst, send, recv, where):
    return pltpu.make_async_remote_copy(src, dst, send, recv, device_id=where, device_id_type=MESH)


def near_peers(teams, j):
    if teams == 4:
        return [j + 1 - 2 * lax.rem(j, 2), lax.rem(j + 2, 4)]
    return [lax.rem(j + step, teams) for step in range(1, teams)]


def all_peers(teams, j):
    if teams == 4:
        return near_peers(teams, j) + [3 - j]
    return near_peers(teams, j)


def spread_own(teams, j, buf, row, height, width, chunk, send, recv):
    view = buf.at[pl.ds(row, height), pl.ds(pl.multiple_of(j * width, 128), width)]
    return [
        remote(view, view, send.at[chunk, turn], recv.at[chunk, turn], {"tp": peer})
        for turn, peer in enumerate(near_peers(teams, j))
    ]


def spread_relay(teams, j, buf, row, height, width, chunk, send, recv):
    if teams != 4:
        return []
    half = height // 2
    across, along = near_peers(teams, j)
    first = buf.at[pl.ds(row, half), pl.ds(pl.multiple_of(across * width, 128), width)]
    second = buf.at[pl.ds(row + half, half), pl.ds(pl.multiple_of(along * width, 128), width)]
    return [
        remote(first, first, send.at[chunk, 2], recv.at[chunk, 2], {"tp": along}),
        remote(second, second, send.at[chunk, 3], recv.at[chunk, 3], {"tp": across}),
    ]


def nt(a, b, precision=None):
    return lax.dot_general(
        a, b, (((1,), (1,)), ((), ())), precision=precision, preferred_element_type=f32
    )


def kernel(
    groups, teams, heads, reach, cap, each, chunks,
    *refs,
):
    inputs, (out, *refs) = refs[:17], refs[17:]
    locals_, refs = refs[:17], refs[17:]
    (
        key, value, forget_t, entry_t, extra_t, docs, choice_t, weight_t, query, gate_out, head_gain, stream, row_gain,
        wo, gate, up, down,
    ) = locals_
    (
        table, kbuf, vbuf, tbuf, cell, ssq, scales, scales_in, chooser, comb, resid, normed, packed, rows, hidden,
        result, returned,
        load_sem, k_send, k_recv, v_send, v_recv, f_send, m_send, m_recv, c_send, c_recv, s_send, s_recv,
        n_send, n_recv, z_send, z_recv, t_send, t_recv, h_send, h_recv, r_send, r_recv,
    ) = refs
    g, j = lax.axis_index("sp"), lax.axis_index("tp")
    tokens, width = stream.shape
    hide = gate.shape[1]
    span = heads * HD
    slots = groups * cap
    tall = each * cap
    model = width * teams
    loads = [
        pltpu.make_async_copy(
            there.at[0] if len(there.shape) > len(here.shape) else there, here, load_sem.at[i]
        )
        for i, (there, here) in enumerate(zip(inputs, locals_))
    ]
    for load in loads:
        load.start()
    barrier = pltpu.get_barrier_semaphore()
    for step in range(1, groups):
        pl.semaphore_signal(
            barrier, inc=1, device_id={"sp": lax.rem(g + step, groups)}, device_id_type=MESH
        )
    peers = all_peers(teams, j)
    for peer in peers:
        pl.semaphore_signal(barrier, inc=1, device_id={"tp": peer}, device_id_type=MESH)
    table[...] = jnp.zeros_like(table)
    for load in loads[:8]:
        load.wait()
    forget = forget_t[...]
    table[0:heads, :] = (
        jnp.minimum(forget, 0.0) - jnp.log1p(jnp.exp(-jnp.abs(forget))) + extra_t[...]
    )
    table[SUB : SUB + heads, :] = entry_t[...]
    table[2 * SUB : 2 * SUB + 1, :] = docs[...].astype(f32)
    table[2 * SUB + 1 : 2 * SUB + 1 + TOPK, :] = choice_t[...].astype(f32)
    table[2 * SUB + 1 + TOPK : 2 * SUB + 1 + 2 * TOPK, :] = weight_t[...]
    pl.semaphore_wait(barrier, groups - 1 + len(peers))

    def send_table(r):
        return remote(table, tbuf.at[r - 1], m_send.at[r - 1], m_recv.at[r - 1], {"sp": g + r})

    def send_pair(r, h):
        cols = pl.ds(h * HD, HD)
        return [
            remote(key.at[:, cols], kbuf.at[r - 1, :, cols], k_send.at[r - 1, h], k_recv.at[r - 1, h], {"sp": g + r}),
            remote(value.at[:, cols], vbuf.at[r - 1, :, cols], v_send.at[r - 1, h], v_recv.at[r - 1, h], {"sp": g + r}),
        ]

    for r in range(1, reach + 1):

        @pl.when(g + r < groups)
        def _(r=r):
            send_table(r).start()

    shared = groups == 8

    def sends(r):
        return (g + r < groups) & (lax.rem(g, 2) == 0) if shared and r == 2 else g + r < groups

    hands_on = (lax.rem(g, 2) == 0) & (g >= 2)

    def hand_on(h):
        cols = pl.ds(h * HD, HD)
        return [
            remote(kbuf.at[0, :, cols], kbuf.at[1, :, cols], f_send.at[0, h], k_recv.at[1, h], {"sp": g + 1}),
            remote(vbuf.at[0, :, cols], vbuf.at[1, :, cols], f_send.at[1, h], v_recv.at[1, h], {"sp": g + 1}),
        ]

    for h in range(heads):
        for r in range(1, reach + 1):

            @pl.when(sends(r))
            def _(r=r, h=h):
                for copy in send_pair(r, h):
                    copy.start()

    for r in range(1, reach + 1):

        @pl.when(g < r)
        def _(r=r):
            kbuf[r - 1] = jnp.zeros_like(kbuf[r - 1])
            vbuf[r - 1] = jnp.zeros_like(vbuf[r - 1])
            tbuf[r - 1] = jnp.full(tbuf.shape[1:], -1.0, f32)

    down_iota = lax.broadcasted_iota(jnp.int32, (tokens, tokens), 0)
    across_iota = lax.broadcasted_iota(jnp.int32, (tokens, tokens), 1)
    causal = across_iota <= down_iota
    lower = causal.astype(f32)
    upper = (down_iota <= across_iota).astype(f32)
    strict = (down_iota < across_iota).astype(bf16)
    eye = (down_iota == across_iota).astype(f32)
    misc = table[2 * SUB : 3 * SUB, :]
    columns = nt(eye, misc, HIGHEST)
    expert_pad = -(-groups // SUB) * SUB
    expert_iota = lax.broadcasted_iota(jnp.int32, (expert_pad, tokens), 0).astype(f32)
    member = jnp.zeros((expert_pad, tokens), f32)
    weighted = jnp.zeros((expert_pad, tokens), f32)
    for ordinal in range(TOPK):
        chosen = expert_iota == misc[1 + ordinal : 2 + ordinal, :]
        member = member + jnp.where(chosen, 1.0, 0.0)
        weighted = weighted + jnp.where(
            chosen, misc[1 + TOPK + ordinal : 2 + TOPK + ordinal, :], 0.0
        )
    rank = jnp.dot(member.astype(bf16), strict, preferred_element_type=f32)
    rank = jnp.where(member > 0.5, rank, -1.0)
    cap_iota = lax.broadcasted_iota(jnp.int32, (cap, tokens), 0).astype(f32)
    for e in range(groups):
        chooser[e * cap : (e + 1) * cap, :] = jnp.where(
            cap_iota == rank[e : e + 1, :], 1.0, 0.0
        ).astype(bf16)
    slot_line = lax.broadcasted_iota(jnp.int32, (1, slots), 1).astype(f32)
    expert_line = jnp.floor((slot_line + 0.5) * (1.0 / cap))
    place_line = slot_line - expert_line * cap
    expand = (
        lax.broadcasted_iota(jnp.int32, (expert_pad, slots), 0).astype(f32) == expert_line
    ).astype(f32)
    rank_wide = jnp.dot(nt(eye, rank), expand, preferred_element_type=f32)
    weight_wide = jnp.dot(
        nt(eye, weighted, HIGHEST), expand, precision=HIGHEST, preferred_element_type=f32
    )
    comb[...] = jnp.where(rank_wide == place_line, weight_wide, 0.0).astype(bf16)

    decay = table[0:SUB, :]
    entry = table[SUB : 2 * SUB, :]
    doc_col = columns[:, 0:1]
    own_mask = causal & (doc_col == misc[0:1, :])
    cum_col = nt(lower, decay, HIGHEST)
    cum_row = jnp.dot(decay, upper, precision=HIGHEST, preferred_element_type=f32)
    carry = nt(own_mask.astype(f32), decay, HIGHEST)
    masks, terms = [own_mask], [entry - cum_row]

    for r in range(1, reach + 1):

        @pl.when(g >= r)
        def _(r=r):
            send_table(r).wait_recv()

    behind = jnp.zeros((SUB, 1), f32)
    for r in range(1, reach + 1):
        decay_r = tbuf[r - 1, 0:SUB, :]
        mask_r = doc_col == tbuf[r - 1, 2 * SUB : 2 * SUB + 1, :]
        cum_r = jnp.dot(decay_r, upper, precision=HIGHEST, preferred_element_type=f32)
        total_r = cum_r[:, tokens - 1 : tokens]
        terms.append(tbuf[r - 1, SUB : 2 * SUB, :] + ((total_r - cum_r) + behind))
        behind = behind + total_r
        carry = carry + nt(mask_r.astype(f32), decay_r, HIGHEST)
        masks.append(mask_r)

    for load in loads[8:13]:
        load.wait()

    def cell_copies(h):
        view = cell.at[:, pl.ds(pl.multiple_of(j * span + h * HD, 128), HD)]
        return [
            remote(view, view, c_send.at[h, turn], c_recv.at[h, turn], {"tp": peer})
            for turn, peer in enumerate(peers)
        ]

    for h in range(heads):
        cols = slice(h * HD, (h + 1) * HD)
        for r in range(1, reach + 1):

            @pl.when(g >= r)
            def _(r=r, h=h):
                for copy in send_pair(r, h):
                    copy.wait_recv()

            if shared and r == 1:

                @pl.when(hands_on)
                def _(h=h):
                    for copy in hand_on(h):
                        copy.start()

        q_h = query[:, cols]
        keys = [key[:, cols]] + [kbuf[r, :, cols] for r in range(reach)]
        values = [value[:, cols]] + [vbuf[r, :, cols] for r in range(reach)]
        peak = carry[:, h : h + 1]
        logs = []
        for mask, term in zip(masks, terms):
            log = jnp.where(mask, cum_col[:, h : h + 1] + term[h : h + 1, :], LOW_LOG)
            peak = jnp.maximum(peak, jnp.max(log, axis=1, keepdims=True))
            logs.append(log)
        denom = jnp.zeros((tokens, 1), f32)
        numer = jnp.zeros((tokens, HD), f32)
        for log, k_b, v_b in zip(logs, keys, values):
            score = nt(q_h, k_b) * (HD ** -0.5) * jnp.exp(log - peak)
            denom = denom + jnp.sum(score, axis=1, keepdims=True)
            numer = numer + jnp.dot(score.astype(bf16), v_b, preferred_element_type=f32)
        value_h = numer / jnp.maximum(jnp.abs(denom), jnp.exp(-peak))
        value_h = value_h * jax.nn.sigmoid(gate_out[:, cols].astype(f32))
        square = jnp.sum(value_h * value_h, axis=1, keepdims=True) * (1.0 / HD)
        value_h = value_h * lax.rsqrt(square + EPSILON) * head_gain[:, cols]
        cell[:, pl.ds(pl.multiple_of(j * span + h * HD, 128), HD)] = value_h.astype(bf16)
        for copy in cell_copies(h):
            copy.start()

    loads[13].wait()
    half = max(1, heads // 2)
    projected = stream[...].astype(f32)
    for first in range(0, heads, half):
        for h in range(first, first + half):
            for copy in cell_copies(h):
                copy.wait_recv()
        for p in range(teams):
            piece = slice(p * span + first * HD, p * span + (first + half) * HD)
            projected = projected + jnp.dot(cell[:, piece], wo[piece, :], preferred_element_type=f32)
    resid[...] = projected.astype(bf16)
    rows_f = resid[...].astype(f32)
    squares = jnp.sum(rows_f * rows_f, axis=1, keepdims=True)
    ssq[j] = jnp.broadcast_to(squares, (tokens, tokens)).T[0:SUB, :]

    def square_copies():
        return [
            remote(ssq.at[j], ssq.at[j], s_send.at[turn], s_recv.at[turn], {"tp": peer})
            for turn, peer in enumerate(peers)
        ]

    for copy in square_copies():
        copy.start()
    normed[...] = (rows_f * row_gain[...].astype(f32).reshape(1, width)).astype(bf16)
    own = pl.ds(pl.multiple_of(g * cap, cap), cap)
    mine = pl.ds(pl.multiple_of(j * width, 128), width)
    block = g // each

    def chunk_of(k):
        if groups != 8:
            return lax.rem(block + k, chunks)
        chip, side = g // 2, lax.rem(g, 2)
        steps = [(step, turn) for step, turn in ORDER if turn < 2 // each]
        at, turn = steps[0]
        for i, (step_i, turn_i) in enumerate(steps[1:]):
            at = jnp.where(k == i + 1, step_i, at)
            turn = jnp.where(k == i + 1, turn_i, turn)
        pair = chip + 1 - 2 * lax.rem(chip, 2)
        there = jnp.where(
            at == 0, chip, jnp.where(at == 1, pair, jnp.where(at == 2, lax.rem(chip + 2, 4), 3 - chip))
        )
        if each == 2:
            return there
        return 2 * there + lax.rem(side + turn, 2)

    def slot_rows(e):
        return pl.ds(pl.multiple_of(e * cap, cap), cap)

    def dispatch(target):
        return remote(
            packed.at[slot_rows(target)], rows.at[own, mine], z_send.at[target], z_recv.at[g], {"sp": target}
        )

    def give_back(target):
        return remote(
            result.at[slot_rows(target)], returned.at[own], r_send.at[target], r_recv.at[g], {"sp": target}
        )

    def over_others(body):
        def one(k, carry_):
            c = chunk_of(k)
            for p in range(each):
                target = c * each + p

                @pl.when(target != g)
                def _():
                    body(target)

            return carry_

        lax.fori_loop(0, chunks, one, 0)

    lead = 3
    if groups == 8:
        lead = jnp.where((g >= 2) & (g < 6), 3, 2)

    def send_chunk(c):
        for p in range(each):
            target = c * each + p

            @pl.when(target != g)
            def _():
                dispatch(target).start()

    def pack(k, carry_):
        c = chunk_of(k)
        at = pl.ds(pl.multiple_of(c * tall, tall), tall)
        packed[at, :] = jnp.dot(chooser[at, :], normed[...], preferred_element_type=f32).astype(bf16)

        @pl.when(k == 0)
        def _():
            rows[own, mine] = packed[own, :]

        @pl.when(k <= lead)
        def _():
            send_chunk(c)

        @pl.when(k == 0)
        def _():
            start_spread(c)

        return carry_


    def row_of(c):
        return pl.multiple_of(c * tall, tall)

    def start_spread(c):
        for p in range(each):
            source = c * each + p

            @pl.when(source != g)
            def _():
                place = rows.at[slot_rows(source), mine]
                remote(place, place, z_send.at[source], z_recv.at[source], {"sp": source}).wait_recv()

        for copy in spread_own(teams, j, rows, row_of(c), tall, width, c, t_send, t_recv):
            copy.start()

    def finish(c):
        row = row_of(c)
        for copy in spread_relay(teams, j, hidden, row, tall, hide, c, h_send, h_recv):
            copy.wait_recv()
        result[pl.ds(row, tall), :] = jnp.dot(
            hidden[pl.ds(row, tall), :], down[...], preferred_element_type=f32
        ).astype(bf16)
        for p in range(each):
            target = c * each + p

            @pl.when(target != g)
            def _():
                give_back(target).start()

            @pl.when(target == g)
            def _():
                returned[own, :] = result[own, :]

    def hidden_relay(c):
        row = row_of(c)
        for copy in spread_own(teams, j, hidden, row, tall, hide, c, h_send, h_recv):
            copy.wait_recv()
        for copy in spread_relay(teams, j, hidden, row, tall, hide, c, h_send, h_recv):
            copy.start()

    lax.fori_loop(0, chunks, pack, 0)
    for copy in square_copies():
        copy.wait_recv()
    total = ssq[0]
    for p in range(1, teams):
        total = total + ssq[p]
    scale = lax.rsqrt(total * (1.0 / model) + EPSILON)
    slot_scale = nt(scale, chooser[...].astype(f32), HIGHEST)
    for e in range(groups):
        scales[e, :, 0:cap] = slot_scale[:, e * cap : (e + 1) * cap]
    scales_in[g] = scales[g]

    def scale_copy(target):
        return remote(scales.at[target], scales_in.at[g], n_send.at[target], n_recv.at[g], {"sp": target})

    over_others(lambda target: scale_copy(target).start())
    for load in loads[14:]:
        load.wait()

    def stage(k, carry_):
        @pl.when((k >= 1) & (k + lead < chunks))
        def _():
            send_chunk(chunk_of(k + lead))

        @pl.when(k < chunks - 1)
        def _():
            start_spread(chunk_of(k + 1))

        @pl.when(k < chunks)
        def _():
            c = chunk_of(k)
            row = row_of(c)
            for copy in spread_own(teams, j, rows, row, tall, width, c, t_send, t_recv):
                copy.wait_recv()
            for copy in spread_relay(teams, j, rows, row, tall, width, c, t_send, t_recv):
                copy.start()

        @pl.when((k >= 1) & (k < chunks + 1))
        def _():
            c = chunk_of(k - 1)
            row = row_of(c)
            for copy in spread_relay(teams, j, rows, row, tall, width, c, t_send, t_recv):
                copy.wait_recv()
            columns_ = []
            for p in range(each):
                source = c * each + p

                @pl.when(source != g)
                def _():
                    place = scales_in.at[source]
                    remote(place, place, n_send.at[source], n_recv.at[source], {"sp": source}).wait_recv()

                line = scales_in[source][0:1, :]
                columns_.append(jnp.broadcast_to(line, (128, 128)).T[0:cap, 0:1])
            factor = columns_[0] if each == 1 else jnp.concatenate(columns_, axis=0)
            block_rows = rows[pl.ds(row, tall), :]
            opened = jnp.dot(block_rows, gate[...], preferred_element_type=f32) * factor
            raised = jnp.dot(block_rows, up[...], preferred_element_type=f32) * factor
            made = (opened * jax.nn.sigmoid(opened) * raised).astype(bf16)
            hidden[pl.ds(row, tall), pl.ds(pl.multiple_of(j * hide, 128), hide)] = made
            for copy in spread_own(teams, j, hidden, row, tall, hide, c, h_send, h_recv):
                copy.start()

        @pl.when((k >= 2) & (k < chunks + 2))
        def _():
            hidden_relay(chunk_of(k - 2))

        @pl.when(k >= 3)
        def _():
            finish(chunk_of(k - 3))

        return carry_

    lax.fori_loop(0, chunks + 3, stage, 0)

    def await_back(source):
        place = returned.at[slot_rows(source)]
        remote(place, place, r_send.at[source], r_recv.at[source], {"sp": source}).wait_recv()

    over_others(await_back)
    mixed = jnp.dot(comb[...], returned[...], preferred_element_type=f32)
    out[...] = (resid[...].astype(f32) + mixed).astype(bf16)

    for r in range(1, reach + 1):

        @pl.when(g + r < groups)
        def _(r=r):
            send_table(r).wait_send()

        @pl.when(sends(r))
        def _(r=r):
            for h in range(heads):
                for copy in send_pair(r, h):
                    copy.wait_send()

    if shared:

        @pl.when(hands_on)
        def _():
            for h in range(heads):
                for copy in hand_on(h):
                    copy.wait_send()

    for h in range(heads):
        for copy in cell_copies(h):
            copy.wait_send()
    for copy in square_copies():
        copy.wait_send()
    over_others(lambda target: scale_copy(target).wait_send())
    over_others(lambda target: dispatch(target).wait_send())
    over_others(lambda target: give_back(target).wait_send())

    def drain(c, carry_):
        row = row_of(c)
        for spread in (spread_own, spread_relay):
            for copy in spread(teams, j, rows, row, tall, width, c, t_send, t_recv):
                copy.wait_send()
            for copy in spread(teams, j, hidden, row, tall, hide, c, h_send, h_recv):
                copy.wait_send()
        return carry_

    lax.fori_loop(0, chunks, drain, 0)


def per_device(
    cell_query_heads,
    cell_key_heads,
    cell_value_heads,
    output_gate_logits,
    input_gate_log,
    forget_gate_logits,
    extra_log_decay,
    documents,
    head_norm_gain,
    stream,
    output_weight,
    expert_norm_gain,
    expert_choice_index,
    routing_weight,
    gate_weight,
    up_weight,
    down_weight,
):
    groups, teams = lax.axis_size("sp"), lax.axis_size("tp")
    tokens, heads = input_gate_log.shape
    span = heads * HD
    width = stream.shape[1]
    _, model, hide = gate_weight.shape
    _, hidden_all, _ = down_weight.shape
    experts_all = groups * gate_weight.shape[0]
    cap = 2 * tokens * TOPK // experts_all
    slots = groups * cap
    each = max(1, min(groups, EACH * 64 // cap))
    chunks = groups // each
    reach = max(1, groups // 4)
    ways = max(4, teams)
    others = teams - 1
    arrays = (
        cell_key_heads,
        cell_value_heads,
        forget_gate_logits.T,
        input_gate_log.T,
        extra_log_decay.T,
        documents[None, :],
        expert_choice_index.T,
        routing_weight.T,
        cell_query_heads,
        output_gate_logits,
        head_norm_gain[None, :],
        stream,
        expert_norm_gain,
        output_weight,
        gate_weight,
        up_weight,
        down_weight,
    )
    vmem = pl.BlockSpec(memory_space=pltpu.VMEM)
    hbm = pl.BlockSpec(memory_space=pl.ANY)
    dma = pltpu.SemaphoreType.DMA
    return pl.pallas_call(
        functools.partial(kernel, groups, teams, heads, reach, cap, each, chunks),
        out_shape=jax.ShapeDtypeStruct((tokens, width), bf16),
        in_specs=[hbm] * 17,
        out_specs=vmem,
        scratch_shapes=[
            *(pltpu.VMEM(a.shape[-2:], a.dtype) for a in arrays),
            pltpu.VMEM((3 * SUB, tokens), f32),
            pltpu.VMEM((reach, tokens, span), bf16),
            pltpu.VMEM((reach, tokens, span), bf16),
            pltpu.VMEM((reach, 3 * SUB, tokens), f32),
            pltpu.VMEM((tokens, teams * span), bf16),
            pltpu.VMEM((teams, SUB, tokens), f32),
            pltpu.VMEM((groups, SUB, 128), f32),
            pltpu.VMEM((groups, SUB, 128), f32),
            pltpu.VMEM((slots, tokens), bf16),
            pltpu.VMEM((tokens, slots), bf16),
            pltpu.VMEM((tokens, width), bf16),
            pltpu.VMEM((tokens, width), bf16),
            pltpu.VMEM((slots, width), bf16),
            pltpu.VMEM((slots, model), bf16),
            pltpu.VMEM((slots, hidden_all), bf16),
            pltpu.VMEM((slots, width), bf16),
            pltpu.VMEM((slots, width), bf16),
            dma((len(arrays),)),
            dma((reach, heads)),
            dma((reach, heads)),
            dma((reach, heads)),
            dma((reach, heads)),
            dma((2, heads)),
            dma((reach,)),
            dma((reach,)),
            dma((heads, others)),
            dma((heads, others)),
            dma((others,)),
            dma((others,)),
            dma((groups,)),
            dma((groups,)),
            dma((groups,)),
            dma((groups,)),
            dma((chunks, ways)),
            dma((chunks, ways)),
            dma((chunks, ways)),
            dma((chunks, ways)),
            dma((groups,)),
            dma((groups,)),
        ],
        compiler_params=pltpu.CompilerParams(
            collective_id=1, has_side_effects=True, vmem_limit_bytes=VMEM_LIMIT
        ),
    )(*arrays)


def solution(mesh):
    placed = (
        P("sp", "tp"),
        P("sp", "tp"),
        P("sp", "tp"),
        P("sp", "tp"),
        P("sp", "tp"),
        P("sp", "tp"),
        P("sp", "tp"),
        P("sp"),
        P("tp"),
        P("sp", "tp"),
        P(None, "tp"),
        P("tp"),
        P("sp", None),
        P("sp", None),
        P("sp", None, "tp"),
        P("sp", None, "tp"),
        P("sp", None, "tp"),
    )
    return jax.shard_map(
        per_device, mesh=mesh, in_specs=placed, out_specs=P("sp", "tp"), check_vma=False
    )
```

```python
import functools

import jax
import jax.numpy as jnp
from jax import lax
from jax.experimental import pallas as pl
from jax.experimental.pallas import tpu as pltpu
from jax.sharding import PartitionSpec as P

HD = 128
TOPK = 2
EPSILON = 1e-06
LOW_LOG = -1e30
HIGHEST = lax.Precision.HIGHEST
MESH = pl.DeviceIdType.MESH
VMEM_LIMIT = 60 * 1024 * 1024
SUB = 8
EACH = 1
PACES = ((-1, -1), (-1, -1), (-1, -1), (-1, -1), (1, 1), (2, 2), (3, 3), (4, 4))
ORDER_MIDDLE = ((0, 0), (1, 0), (2, 0), (2, 1), (3, 0), (3, 1), (1, 1), (0, 1))
ORDER_END = ((0, 0), (0, 1), (2, 0), (1, 0), (2, 1), (3, 0), (3, 1), (1, 1))
f32, bf16 = jnp.float32, jnp.bfloat16


def remote(src, dst, send, recv, where):
    return pltpu.make_async_remote_copy(src, dst, send, recv, device_id=where, device_id_type=MESH)


def near_peers(teams, j):
    if teams == 4:
        return [j + 1 - 2 * lax.rem(j, 2), lax.rem(j + 2, 4)]
    return [lax.rem(j + step, teams) for step in range(1, teams)]


def all_peers(teams, j):
    if teams == 4:
        return near_peers(teams, j) + [3 - j]
    return near_peers(teams, j)


def spread_own(teams, j, buf, row, height, width, chunk, send, recv):
    view = buf.at[pl.ds(row, height), pl.ds(pl.multiple_of(j * width, 128), width)]
    return [
        remote(view, view, send.at[0], recv.at[chunk, 0], {"tp": peer}) for peer in near_peers(teams, j)
    ]


def spread_relay(teams, j, buf, row, height, width, chunk, send, recv):
    if teams != 4:
        return []
    half = height // 2
    across, along = near_peers(teams, j)
    first = buf.at[pl.ds(row, half), pl.ds(pl.multiple_of(across * width, 128), width)]
    second = buf.at[pl.ds(row + half, half), pl.ds(pl.multiple_of(along * width, 128), width)]
    return [
        remote(first, first, send.at[0], recv.at[chunk, 1], {"tp": along}),
        remote(second, second, send.at[0], recv.at[chunk, 1], {"tp": across}),
    ]


def arrived(view, sem, g):
    remote(view, view, sem, sem, {"sp": g}).wait_recv()


def departed(view, sem, g):
    remote(view, view, sem, sem, {"sp": g}).wait_send()


def own_arrived(teams, g, buf, row, height, width, chunk, recv):
    count = 2 if teams == 4 else teams - 1
    arrived(buf.at[pl.ds(row, height), 0 : count * width], recv.at[chunk, 0], g)


def relay_arrived(teams, g, buf, row, height, width, chunk, recv):
    if teams == 4:
        arrived(buf.at[pl.ds(row, height // 2), 0 : 2 * width], recv.at[chunk, 1], g)


def nt(a, b, precision=None):
    return lax.dot_general(
        a, b, (((1,), (1,)), ((), ())), precision=precision, preferred_element_type=f32
    )


def kernel(
    groups, teams, heads, reach, cap, each, chunks,
    *refs,
):
    inputs, (out, *refs) = refs[:17], refs[17:]
    locals_, refs = refs[:17], refs[17:]
    (
        key, value, forget_t, entry_t, extra_t, docs, choice_t, weight_t, query, gate_out, head_gain, stream, row_gain,
        wo, gate, up, down,
    ) = locals_
    (
        table, kvbuf, tbuf, cell, ssq, scales, scales_in, chooser, comb, resid, normed, packed, rows, hidden,
        result, returned,
        load_sem, k_send, k_recv, f_send, m_send, m_recv, c_send, c_recv, s_send, s_recv,
        o_sem, n_send, n_recv, z_send, z_recv, t_send, t_recv, h_send, h_recv, r_send, r_recv,
    ) = refs
    g, j = lax.axis_index("sp"), lax.axis_index("tp")
    other = lax.rem(g + 1, groups)
    tokens, width = stream.shape
    hide = gate.shape[1]
    span = heads * HD
    slots = groups * cap
    tall = each * cap
    model = width * teams
    loads = [
        pltpu.make_async_copy(
            there.at[0] if len(there.shape) > len(here.shape) else there, here, load_sem.at[i]
        )
        for i, (there, here) in enumerate(zip(inputs, locals_))
    ]
    for load in loads:
        load.start()
    barrier = pltpu.get_barrier_semaphore()
    for step in range(1, groups):
        pl.semaphore_signal(
            barrier, inc=1, device_id={"sp": lax.rem(g + step, groups)}, device_id_type=MESH
        )
    peers = all_peers(teams, j)
    for peer in peers:
        pl.semaphore_signal(barrier, inc=1, device_id={"tp": peer}, device_id_type=MESH)
    table[...] = jnp.zeros_like(table)
    for load in loads[:8]:
        load.wait()
    forget = forget_t[...]
    table[0:heads, :] = (
        jnp.minimum(forget, 0.0) - jnp.log1p(jnp.exp(-jnp.abs(forget))) + extra_t[...]
    )
    table[SUB : SUB + heads, :] = entry_t[...]
    table[2 * SUB : 2 * SUB + 1, :] = docs[...].astype(f32)
    table[2 * SUB + 1 : 2 * SUB + 1 + TOPK, :] = choice_t[...].astype(f32)
    table[2 * SUB + 1 + TOPK : 2 * SUB + 1 + 2 * TOPK, :] = weight_t[...]
    pl.semaphore_wait(barrier, groups - 1 + len(peers))

    def send_table(r):
        return remote(table, tbuf.at[r - 1], m_send.at[r - 1], m_recv.at[r - 1], {"sp": g + r})

    def send_pair(r, h):
        cols = pl.ds(h * HD, HD)
        return [
            remote(key.at[:, cols], kvbuf.at[r - 1, 0, :, cols], k_send.at[r - 1], k_recv.at[r - 1, h], {"sp": g + r}),
            remote(value.at[:, cols], kvbuf.at[r - 1, 1, :, cols], k_send.at[r - 1], k_recv.at[r - 1, h], {"sp": g + r}),
        ]

    for r in range(1, reach + 1):

        @pl.when(g + r < groups)
        def _(r=r):
            send_table(r).start()

    shared = groups == 8

    def sends(r):
        return (g + r < groups) & (lax.rem(g, 2) == 0) if shared and r == 2 else g + r < groups

    hands_on = (lax.rem(g, 2) == 0) & (g >= 2)

    def hand_on(h):
        cols = pl.ds(h * HD, HD)
        view = kvbuf.at[0, :, :, cols]
        return [remote(view, kvbuf.at[1, :, :, cols], f_send.at[0], k_recv.at[1, h], {"sp": g + 1})]

    for h in range(heads):
        for r in range(1, reach + 1):

            @pl.when(sends(r))
            def _(r=r, h=h):
                for copy in send_pair(r, h):
                    copy.start()

    for r in range(1, reach + 1):

        @pl.when(g < r)
        def _(r=r):
            kvbuf[r - 1] = jnp.zeros_like(kvbuf[r - 1])
            tbuf[r - 1] = jnp.full(tbuf.shape[1:], -1.0, f32)

    down_iota = lax.broadcasted_iota(jnp.int32, (tokens, tokens), 0)
    across_iota = lax.broadcasted_iota(jnp.int32, (tokens, tokens), 1)
    causal = across_iota <= down_iota
    lower = causal.astype(f32)
    upper = (down_iota <= across_iota).astype(f32)
    strict = (down_iota < across_iota).astype(bf16)
    eye = (down_iota == across_iota).astype(f32)
    misc = table[2 * SUB : 3 * SUB, :]
    columns = nt(eye, misc, HIGHEST)
    expert_pad = -(-groups // SUB) * SUB
    expert_iota = lax.broadcasted_iota(jnp.int32, (expert_pad, tokens), 0).astype(f32)
    member = jnp.zeros((expert_pad, tokens), f32)
    weighted = jnp.zeros((expert_pad, tokens), f32)
    for ordinal in range(TOPK):
        chosen = expert_iota == misc[1 + ordinal : 2 + ordinal, :]
        member = member + jnp.where(chosen, 1.0, 0.0)
        weighted = weighted + jnp.where(
            chosen, misc[1 + TOPK + ordinal : 2 + TOPK + ordinal, :], 0.0
        )
    rank = jnp.dot(member.astype(bf16), strict, preferred_element_type=f32)
    rank = jnp.where(member > 0.5, rank, -1.0)
    cap_iota = lax.broadcasted_iota(jnp.int32, (cap, tokens), 0).astype(f32)
    for e in range(groups):
        chooser[e * cap : (e + 1) * cap, :] = jnp.where(
            cap_iota == rank[e : e + 1, :], 1.0, 0.0
        ).astype(bf16)
    slot_line = lax.broadcasted_iota(jnp.int32, (1, slots), 1).astype(f32)
    expert_line = jnp.floor((slot_line + 0.5) * (1.0 / cap))
    place_line = slot_line - expert_line * cap
    expand = (
        lax.broadcasted_iota(jnp.int32, (expert_pad, slots), 0).astype(f32) == expert_line
    ).astype(f32)
    rank_wide = jnp.dot(nt(eye, rank), expand, preferred_element_type=f32)
    weight_wide = jnp.dot(
        nt(eye, weighted, HIGHEST), expand, precision=HIGHEST, preferred_element_type=f32
    )
    comb[...] = jnp.where(rank_wide == place_line, weight_wide, 0.0).astype(bf16)

    decay = table[0:SUB, :]
    entry = table[SUB : 2 * SUB, :]
    doc_col = columns[:, 0:1]
    own_mask = causal & (doc_col == misc[0:1, :])
    cum_col = nt(lower, decay, HIGHEST)
    cum_row = jnp.dot(decay, upper, precision=HIGHEST, preferred_element_type=f32)
    carry = nt(own_mask.astype(f32), decay, HIGHEST)
    masks, terms = [own_mask], [entry - cum_row]

    for r in range(1, reach + 1):

        @pl.when(g >= r)
        def _(r=r):
            send_table(r).wait_recv()

    behind = jnp.zeros((SUB, 1), f32)
    for r in range(1, reach + 1):
        decay_r = tbuf[r - 1, 0:SUB, :]
        mask_r = doc_col == tbuf[r - 1, 2 * SUB : 2 * SUB + 1, :]
        cum_r = jnp.dot(decay_r, upper, precision=HIGHEST, preferred_element_type=f32)
        total_r = cum_r[:, tokens - 1 : tokens]
        terms.append(tbuf[r - 1, SUB : 2 * SUB, :] + ((total_r - cum_r) + behind))
        behind = behind + total_r
        carry = carry + nt(mask_r.astype(f32), decay_r, HIGHEST)
        masks.append(mask_r)

    for load in loads[8:13]:
        load.wait()

    half = max(1, heads // 2)

    def cell_copies(h):
        view = cell.at[:, pl.ds(pl.multiple_of(j * span + h * HD, 128), HD)]
        return [
            remote(view, view, c_send.at[0], c_recv.at[h // half], {"tp": peer}) for peer in peers
        ]

    for h in range(heads):
        cols = slice(h * HD, (h + 1) * HD)
        for r in range(1, reach + 1):

            @pl.when(g >= r)
            def _(r=r, h=h):
                arrived(kvbuf.at[r - 1, :, :, pl.ds(h * HD, HD)], k_recv.at[r - 1, h], g - r)

            if shared and r == 1:

                @pl.when(hands_on)
                def _(h=h):
                    for copy in hand_on(h):
                        copy.start()

        q_h = query[:, cols]
        keys = [key[:, cols]] + [kvbuf[r, 0, :, cols] for r in range(reach)]
        values = [value[:, cols]] + [kvbuf[r, 1, :, cols] for r in range(reach)]
        peak = carry[:, h : h + 1]
        logs = []
        for mask, term in zip(masks, terms):
            log = jnp.where(mask, cum_col[:, h : h + 1] + term[h : h + 1, :], LOW_LOG)
            peak = jnp.maximum(peak, jnp.max(log, axis=1, keepdims=True))
            logs.append(log)
        denom = jnp.zeros((tokens, 1), f32)
        numer = jnp.zeros((tokens, HD), f32)
        for log, k_b, v_b in zip(logs, keys, values):
            score = nt(q_h, k_b) * (HD ** -0.5) * jnp.exp(log - peak)
            denom = denom + jnp.sum(score, axis=1, keepdims=True)
            numer = numer + jnp.dot(score.astype(bf16), v_b, preferred_element_type=f32)
        value_h = numer / jnp.maximum(jnp.abs(denom), jnp.exp(-peak))
        value_h = value_h * jax.nn.sigmoid(gate_out[:, cols].astype(f32))
        square = jnp.sum(value_h * value_h, axis=1, keepdims=True) * (1.0 / HD)
        value_h = value_h * lax.rsqrt(square + EPSILON) * head_gain[:, cols]
        cell[:, pl.ds(pl.multiple_of(j * span + h * HD, 128), HD)] = value_h.astype(bf16)
        for copy in cell_copies(h):
            copy.start()

    loads[13].wait()
    projected = stream[...].astype(f32)
    for first in range(0, heads, half):
        arrived(cell.at[:, 0 : half * HD * (teams - 1)], c_recv.at[first // half], other)
        for p in range(teams):
            piece = slice(p * span + first * HD, p * span + (first + half) * HD)
            projected = projected + jnp.dot(cell[:, piece], wo[piece, :], preferred_element_type=f32)
    resid[...] = projected.astype(bf16)
    rows_f = resid[...].astype(f32)
    squares = jnp.sum(rows_f * rows_f, axis=1, keepdims=True)
    ssq[j] = jnp.broadcast_to(squares, (tokens, tokens)).T[0:SUB, :]

    def square_copies():
        return [
            remote(ssq.at[j], ssq.at[j], s_send.at[0], s_recv.at[0], {"tp": peer}) for peer in peers
        ]

    for copy in square_copies():
        copy.start()
    normed[...] = (rows_f * row_gain[...].astype(f32).reshape(1, width)).astype(bf16)
    own = pl.ds(pl.multiple_of(g * cap, cap), cap)
    mine = pl.ds(pl.multiple_of(j * width, 128), width)
    block = g // each

    def chunk_of(k):
        if groups != 8:
            return lax.rem(block + k, chunks)
        chip, side = g // 2, lax.rem(g, 2)
        middle = (g >= 2) & (g < 6)

        def picked(order):
            steps = [(step, turn) for step, turn in order if turn < 2 // each]
            at, turn = steps[0]
            for i, (step_i, turn_i) in enumerate(steps[1:]):
                at = jnp.where(k == i + 1, step_i, at)
                turn = jnp.where(k == i + 1, turn_i, turn)
            return at, turn

        at, turn = [jnp.where(middle, mid, end) for mid, end in zip(picked(ORDER_MIDDLE), picked(ORDER_END))]
        pair = chip + 1 - 2 * lax.rem(chip, 2)
        there = jnp.where(
            at == 0, chip, jnp.where(at == 1, pair, jnp.where(at == 2, lax.rem(chip + 2, 4), 3 - chip))
        )
        if each == 2:
            return there
        return 2 * there + lax.rem(side + turn, 2)

    def slot_rows(e):
        return pl.ds(pl.multiple_of(e * cap, cap), cap)

    def dispatch(target):
        return remote(
            packed.at[slot_rows(target)], rows.at[own, mine], z_send.at[0], z_recv.at[g], {"sp": target}
        )

    def give_back(target):
        return remote(
            result.at[slot_rows(target)], returned.at[own], r_send.at[0], r_recv.at[0], {"sp": target}
        )

    def over_others(body):
        def one(k, carry_):
            c = chunk_of(k)
            for p in range(each):
                target = c * each + p

                @pl.when(target != g)
                def _():
                    body(target)

            return carry_

        lax.fori_loop(0, chunks, one, 0)

    lined = groups == 8 and each == 1
    if lined:
        middle = (g >= 2) & (g < 6)
        paces = [jnp.where(middle, mid, end) for mid, end in PACES]
    else:
        paces = [max(-1, k - 3) for k in range(chunks)]

    def issue(now):
        for k, pace in enumerate(paces):

            @pl.when(pace == now)
            def _(k=k):
                send_chunk(chunk_of(k))

    def send_chunk(c):
        for p in range(each):
            target = c * each + p

            @pl.when(target != g)
            def _():
                dispatch(target).start()

    def pack(k, carry_):
        c = chunk_of(k)
        at = pl.ds(pl.multiple_of(c * tall, tall), tall)
        packed[at, :] = jnp.dot(chooser[at, :], normed[...], preferred_element_type=f32).astype(bf16)

        @pl.when(k == 0)
        def _():
            rows[own, mine] = packed[own, :]

        for i, pace in enumerate(paces):

            @pl.when((k == i) & (pace == -1))
            def _():
                send_chunk(c)

        @pl.when(k == 0)
        def _():
            start_spread(c)

        return carry_


    def row_of(c):
        return pl.multiple_of(c * tall, tall)

    def start_spread(c):
        for p in range(each):
            source = c * each + p

            @pl.when(source != g)
            def _():
                place = rows.at[slot_rows(source), mine]
                arrived(place, z_recv.at[source], source)

        for copy in spread_own(teams, j, rows, row_of(c), tall, width, c, t_send, t_recv):
            copy.start()

    def finish(c):
        row = row_of(c)
        relay_arrived(teams, other, hidden, row, tall, hide, c, h_recv)
        result[pl.ds(row, tall), :] = jnp.dot(
            hidden[pl.ds(row, tall), :], down[...], preferred_element_type=f32
        ).astype(bf16)
        for p in range(each):
            target = c * each + p

            @pl.when(target != g)
            def _():
                give_back(target).start()

            @pl.when(target == g)
            def _():
                returned[own, :] = result[own, :]

    def hidden_relay(c):
        row = row_of(c)
        own_arrived(teams, other, hidden, row, tall, hide, c, h_recv)
        for copy in spread_relay(teams, j, hidden, row, tall, hide, c, h_send, h_recv):
            copy.start()

    lax.fori_loop(0, chunks, pack, 0)
    arrived(ssq.at[0 : teams - 1], s_recv.at[0], other)
    total = ssq[0]
    for p in range(1, teams):
        total = total + ssq[p]
    scale = lax.rsqrt(total * (1.0 / model) + EPSILON)
    slot_scale = nt(scale, chooser[...].astype(f32), HIGHEST)
    for e in range(groups):
        scales[e, :, 0:cap] = slot_scale[:, e * cap : (e + 1) * cap]
    scales_in[g] = scales[g]

    def scale_copy(target):
        return remote(scales.at[target], scales_in.at[g], n_send.at[0], n_recv.at[g], {"sp": target})

    over_others(lambda target: scale_copy(target).start())
    for load in loads[14:]:
        load.wait()

    def stage(k, carry_):
        issue(k)

        @pl.when(k < chunks - 1)
        def _():
            start_spread(chunk_of(k + 1))

        @pl.when(k < chunks)
        def _():
            c = chunk_of(k)
            row = row_of(c)
            own_arrived(teams, other, rows, row, tall, width, c, t_recv)
            for copy in spread_relay(teams, j, rows, row, tall, width, c, t_send, t_recv):
                copy.start()

        @pl.when((k >= 1) & (k < chunks + 1))
        def _():
            c = chunk_of(k - 1)
            row = row_of(c)
            relay_arrived(teams, other, rows, row, tall, width, c, t_recv)
            columns_ = []
            for p in range(each):
                source = c * each + p

                @pl.when(source != g)
                def _():
                    place = scales_in.at[source]
                    arrived(place, n_recv.at[source], source)

                line = scales_in[source][0:1, :]
                columns_.append(jnp.broadcast_to(line, (128, 128)).T[0:cap, 0:1])
            factor = columns_[0] if each == 1 else jnp.concatenate(columns_, axis=0)
            block_rows = rows[pl.ds(row, tall), :]
            opened = jnp.dot(block_rows, gate[...], preferred_element_type=f32) * factor
            raised = jnp.dot(block_rows, up[...], preferred_element_type=f32) * factor
            made = (opened * jax.nn.sigmoid(opened) * raised).astype(bf16)
            hidden[pl.ds(row, tall), pl.ds(pl.multiple_of(j * hide, 128), hide)] = made
            for copy in spread_own(teams, j, hidden, row, tall, hide, c, h_send, h_recv):
                copy.start()

        @pl.when((k >= 2) & (k < chunks + 2))
        def _():
            hidden_relay(chunk_of(k - 2))

        @pl.when(k >= 3)
        def _():
            finish(chunk_of(k - 3))

        return carry_

    lax.fori_loop(0, chunks + 3, stage, 0)

    for r in range(1, reach + 1):

        @pl.when(g + r < groups)
        def _(r=r):
            send_table(r).wait_send()

        @pl.when(sends(r))
        def _(r=r):
            departed(kvbuf.at[r - 1], k_send.at[r - 1], g + r)

    if shared:

        @pl.when(hands_on)
        def _():
            departed(kvbuf.at[0], f_send.at[0], g + 1)

    departed(cell.at[:, 0 : span * (teams - 1)], c_send.at[0], other)
    departed(ssq.at[0 : teams - 1], s_send.at[0], other)
    departed(scales.at[0 : groups - 1], n_send.at[0], other)
    departed(packed.at[0 : (groups - 1) * cap], z_send.at[0], other)
    departed(rows.at[:, 0 : (teams - 1) * width], t_send.at[0], other)
    departed(hidden.at[:, 0 : (teams - 1) * hide], h_send.at[0], other)
    arrived(returned.at[0 : (groups - 1) * cap], r_recv.at[0], other)
    part = width // 2 if width % 256 == 0 else width
    stores = []
    for i in range(width // part):
        cut = slice(i * part, (i + 1) * part)
        mixed = jnp.dot(comb[...], returned[:, cut], preferred_element_type=f32)
        resid[:, cut] = (resid[:, cut].astype(f32) + mixed).astype(bf16)
        stores.append(pltpu.make_async_copy(resid.at[:, cut], out.at[:, cut], o_sem.at[i]))
        stores[-1].start()
    departed(result.at[0 : (groups - 1) * cap], r_send.at[0], other)
    for store in stores:
        store.wait()


def per_device(
    cell_query_heads,
    cell_key_heads,
    cell_value_heads,
    output_gate_logits,
    input_gate_log,
    forget_gate_logits,
    extra_log_decay,
    documents,
    head_norm_gain,
    stream,
    output_weight,
    expert_norm_gain,
    expert_choice_index,
    routing_weight,
    gate_weight,
    up_weight,
    down_weight,
):
    groups, teams = lax.axis_size("sp"), lax.axis_size("tp")
    tokens, heads = input_gate_log.shape
    span = heads * HD
    width = stream.shape[1]
    _, model, hide = gate_weight.shape
    _, hidden_all, _ = down_weight.shape
    experts_all = groups * gate_weight.shape[0]
    cap = 2 * tokens * TOPK // experts_all
    slots = groups * cap
    each = max(1, min(groups, EACH * 64 // cap))
    chunks = groups // each
    reach = max(1, groups // 4)
    arrays = (
        cell_key_heads,
        cell_value_heads,
        forget_gate_logits.T,
        input_gate_log.T,
        extra_log_decay.T,
        documents[None, :],
        expert_choice_index.T,
        routing_weight.T,
        cell_query_heads,
        output_gate_logits,
        head_norm_gain[None, :],
        stream,
        expert_norm_gain,
        output_weight,
        gate_weight,
        up_weight,
        down_weight,
    )
    hbm = pl.BlockSpec(memory_space=pl.ANY)
    dma = pltpu.SemaphoreType.DMA
    return pl.pallas_call(
        functools.partial(kernel, groups, teams, heads, reach, cap, each, chunks),
        out_shape=jax.ShapeDtypeStruct((tokens, width), bf16),
        in_specs=[hbm] * 17,
        out_specs=hbm,
        scratch_shapes=[
            *(pltpu.VMEM(a.shape[-2:], a.dtype) for a in arrays),
            pltpu.VMEM((3 * SUB, tokens), f32),
            pltpu.VMEM((reach, 2, tokens, span), bf16),
            pltpu.VMEM((reach, 3 * SUB, tokens), f32),
            pltpu.VMEM((tokens, teams * span), bf16),
            pltpu.VMEM((teams, SUB, tokens), f32),
            pltpu.VMEM((groups, SUB, 128), f32),
            pltpu.VMEM((groups, SUB, 128), f32),
            pltpu.VMEM((slots, tokens), bf16),
            pltpu.VMEM((tokens, slots), bf16),
            pltpu.VMEM((tokens, width), bf16),
            pltpu.VMEM((tokens, width), bf16),
            pltpu.VMEM((slots, width), bf16),
            pltpu.VMEM((slots, model), bf16),
            pltpu.VMEM((slots, hidden_all), bf16),
            pltpu.VMEM((slots, width), bf16),
            pltpu.VMEM((slots, width), bf16),
            dma((len(arrays),)),
            dma((reach,)),
            dma((reach, heads)),
            dma((1,)),
            dma((reach,)),
            dma((reach,)),
            dma((1,)),
            dma((2,)),
            dma((1,)),
            dma((1,)),
            dma((2,)),
            dma((1,)),
            dma((groups,)),
            dma((1,)),
            dma((groups,)),
            dma((1,)),
            dma((chunks, 2)),
            dma((1,)),
            dma((chunks, 2)),
            dma((1,)),
            dma((1,)),
        ],
        compiler_params=pltpu.CompilerParams(
            collective_id=1, has_side_effects=True, vmem_limit_bytes=VMEM_LIMIT
        ),
    )(*arrays)


def solution(mesh):
    placed = (
        P("sp", "tp"),
        P("sp", "tp"),
        P("sp", "tp"),
        P("sp", "tp"),
        P("sp", "tp"),
        P("sp", "tp"),
        P("sp", "tp"),
        P("sp"),
        P("tp"),
        P("sp", "tp"),
        P(None, "tp"),
        P("tp"),
        P("sp", None),
        P("sp", None),
        P("sp", None, "tp"),
        P("sp", None, "tp"),
        P("sp", None, "tp"),
    )
    return jax.shard_map(
        per_device, mesh=mesh, in_specs=placed, out_specs=P("sp", "tp"), check_vma=False
    )
```

```python
import functools

import jax
import jax.numpy as jnp
from jax import lax
from jax.experimental import pallas as pl
from jax.experimental.pallas import tpu as pltpu
from jax.sharding import PartitionSpec as P

HD = 128
TOPK = 2
EPSILON = 1e-06
LOW_LOG = -1e30
HIGHEST = lax.Precision.HIGHEST
MESH = pl.DeviceIdType.MESH
VMEM_LIMIT = 60 * 1024 * 1024
SUB = 8
EACH = 1
PACES = ((-1, -1), (-1, -1), (-1, -1), (-1, -1), (1, 1), (2, 2), (3, 3), (4, 4))
ORDER_MIDDLE = ((0, 0), (1, 0), (2, 0), (2, 1), (3, 0), (3, 1), (1, 1), (0, 1))
ORDER_END = ((0, 0), (0, 1), (2, 0), (1, 0), (2, 1), (3, 0), (3, 1), (1, 1))
f32, bf16 = jnp.float32, jnp.bfloat16


def remote(src, dst, send, recv, where):
    return pltpu.make_async_remote_copy(src, dst, send, recv, device_id=where, device_id_type=MESH)


def near_peers(teams, j):
    if teams == 4:
        return [j + 1 - 2 * lax.rem(j, 2), lax.rem(j + 2, 4)]
    return [lax.rem(j + step, teams) for step in range(1, teams)]


def all_peers(teams, j):
    if teams == 4:
        return near_peers(teams, j) + [3 - j]
    return near_peers(teams, j)


def spread_own(teams, j, buf, row, height, width, chunk, send, recv):
    view = buf.at[pl.ds(row, height), pl.ds(pl.multiple_of(j * width, 128), width)]
    return [
        remote(view, view, send.at[0], recv.at[chunk, 0], {"tp": peer}) for peer in near_peers(teams, j)
    ]


def spread_relay(teams, j, buf, row, height, width, chunk, send, recv):
    if teams != 4:
        return []
    half = height // 2
    across, along = near_peers(teams, j)
    first = buf.at[pl.ds(row, half), pl.ds(pl.multiple_of(across * width, 128), width)]
    second = buf.at[pl.ds(row + half, half), pl.ds(pl.multiple_of(along * width, 128), width)]
    return [
        remote(first, first, send.at[0], recv.at[chunk, 1], {"tp": along}),
        remote(second, second, send.at[0], recv.at[chunk, 1], {"tp": across}),
    ]


def arrived(view, sem, g):
    remote(view, view, sem, sem, {"sp": g}).wait_recv()


def departed(view, sem, g):
    remote(view, view, sem, sem, {"sp": g}).wait_send()


def own_arrived(teams, g, buf, row, height, width, chunk, recv):
    count = 2 if teams == 4 else teams - 1
    arrived(buf.at[pl.ds(row, height), 0 : count * width], recv.at[chunk, 0], g)


def relay_arrived(teams, g, buf, row, height, width, chunk, recv):
    if teams == 4:
        arrived(buf.at[pl.ds(row, height // 2), 0 : 2 * width], recv.at[chunk, 1], g)


def nt(a, b, precision=None):
    return lax.dot_general(
        a, b, (((1,), (1,)), ((), ())), precision=precision, preferred_element_type=f32
    )


def kernel(
    groups, teams, heads, reach, cap, each, chunks,
    *refs,
):
    inputs, (out, *refs) = refs[:17], refs[17:]
    locals_, refs = refs[:17], refs[17:]
    (
        key, value, forget_t, entry_t, extra_t, docs, choice_t, weight_t, query, gate_out, head_gain, stream, row_gain,
        wo, gate, up, down,
    ) = locals_
    (
        table, kvbuf, tbuf, cell, ssq, scales, scales_in, chooser, comb, resid, normed, packed, rows, hidden,
        result, returned,
        load_sem, k_send, k_recv, f_send, m_send, m_recv, c_send, c_recv, s_send, s_recv,
        o_sem, n_send, n_recv, z_send, z_recv, t_send, t_recv, h_send, h_recv, r_send, r_recv,
    ) = refs
    g, j = lax.axis_index("sp"), lax.axis_index("tp")
    other = lax.rem(g + 1, groups)
    tokens, width = stream.shape
    hide = gate.shape[1]
    span = heads * HD
    slots = groups * cap
    tall = each * cap
    model = width * teams
    loads = [
        pltpu.make_async_copy(
            there.at[0] if len(there.shape) > len(here.shape) else there, here, load_sem.at[i]
        )
        for i, (there, here) in enumerate(zip(inputs, locals_))
    ]
    for load in loads:
        load.start()
    barrier = pltpu.get_barrier_semaphore()
    for step in range(1, groups):
        pl.semaphore_signal(
            barrier, inc=1, device_id={"sp": lax.rem(g + step, groups)}, device_id_type=MESH
        )
    peers = all_peers(teams, j)
    for peer in peers:
        pl.semaphore_signal(barrier, inc=1, device_id={"tp": peer}, device_id_type=MESH)
    table[...] = jnp.zeros_like(table)
    for load in loads[:8]:
        load.wait()
    forget = forget_t[...]
    table[0:heads, :] = (
        jnp.minimum(forget, 0.0) - jnp.log1p(jnp.exp(-jnp.abs(forget))) + extra_t[...]
    )
    table[SUB : SUB + heads, :] = entry_t[...]
    table[2 * SUB : 2 * SUB + 1, :] = docs[...].astype(f32)
    table[2 * SUB + 1 : 2 * SUB + 1 + TOPK, :] = choice_t[...].astype(f32)
    table[2 * SUB + 1 + TOPK : 2 * SUB + 1 + 2 * TOPK, :] = weight_t[...]
    pl.semaphore_wait(barrier, groups - 1 + len(peers))

    def send_table(r):
        return remote(table, tbuf.at[r - 1], m_send.at[r - 1], m_recv.at[r - 1], {"sp": g + r})

    def send_pair(r, h):
        cols = pl.ds(h * HD, HD)
        return [
            remote(key.at[:, cols], kvbuf.at[r - 1, 0, :, cols], k_send.at[r - 1], k_recv.at[r - 1, h], {"sp": g + r}),
            remote(value.at[:, cols], kvbuf.at[r - 1, 1, :, cols], k_send.at[r - 1], k_recv.at[r - 1, h], {"sp": g + r}),
        ]

    for r in range(1, reach + 1):

        @pl.when(g + r < groups)
        def _(r=r):
            send_table(r).start()

    shared = groups == 8

    def sends(r):
        return (g + r < groups) & (lax.rem(g, 2) == 0) if shared and r == 2 else g + r < groups

    hands_on = (lax.rem(g, 2) == 0) & (g >= 2)

    def hand_on(h):
        cols = pl.ds(h * HD, HD)
        view = kvbuf.at[0, :, :, cols]
        return [remote(view, kvbuf.at[1, :, :, cols], f_send.at[0], k_recv.at[1, h], {"sp": g + 1})]

    for h in range(heads):
        for r in range(1, reach + 1):

            @pl.when(sends(r))
            def _(r=r, h=h):
                for copy in send_pair(r, h):
                    copy.start()

    for r in range(1, reach + 1):

        @pl.when(g < r)
        def _(r=r):
            kvbuf[r - 1] = jnp.zeros_like(kvbuf[r - 1])
            tbuf[r - 1] = jnp.full(tbuf.shape[1:], -1.0, f32)

    down_iota = lax.broadcasted_iota(jnp.int32, (tokens, tokens), 0)
    across_iota = lax.broadcasted_iota(jnp.int32, (tokens, tokens), 1)
    causal = across_iota <= down_iota
    lower = causal.astype(f32)
    upper = (down_iota <= across_iota).astype(f32)
    strict = (down_iota < across_iota).astype(bf16)
    eye = (down_iota == across_iota).astype(f32)
    misc = table[2 * SUB : 3 * SUB, :]
    columns = nt(eye, misc, HIGHEST)
    expert_pad = -(-groups // SUB) * SUB
    expert_iota = lax.broadcasted_iota(jnp.int32, (expert_pad, tokens), 0).astype(f32)
    member = jnp.zeros((expert_pad, tokens), f32)
    weighted = jnp.zeros((expert_pad, tokens), f32)
    for ordinal in range(TOPK):
        chosen = expert_iota == misc[1 + ordinal : 2 + ordinal, :]
        member = member + jnp.where(chosen, 1.0, 0.0)
        weighted = weighted + jnp.where(
            chosen, misc[1 + TOPK + ordinal : 2 + TOPK + ordinal, :], 0.0
        )
    rank = jnp.dot(member.astype(bf16), strict, preferred_element_type=f32)
    rank = jnp.where(member > 0.5, rank, -1.0)
    cap_iota = lax.broadcasted_iota(jnp.int32, (cap, tokens), 0).astype(f32)
    for e in range(groups):
        chooser[e * cap : (e + 1) * cap, :] = jnp.where(
            cap_iota == rank[e : e + 1, :], 1.0, 0.0
        ).astype(bf16)
    slot_line = lax.broadcasted_iota(jnp.int32, (1, slots), 1).astype(f32)
    expert_line = jnp.floor((slot_line + 0.5) * (1.0 / cap))
    place_line = slot_line - expert_line * cap
    expand = (
        lax.broadcasted_iota(jnp.int32, (expert_pad, slots), 0).astype(f32) == expert_line
    ).astype(f32)
    rank_wide = jnp.dot(nt(eye, rank), expand, preferred_element_type=f32)
    weight_wide = jnp.dot(
        nt(eye, weighted, HIGHEST), expand, precision=HIGHEST, preferred_element_type=f32
    )
    comb[...] = jnp.where(rank_wide == place_line, weight_wide, 0.0).astype(bf16)

    decay = table[0:SUB, :]
    entry = table[SUB : 2 * SUB, :]
    doc_col = columns[:, 0:1]
    own_mask = causal & (doc_col == misc[0:1, :])
    cum_col = nt(lower, decay, HIGHEST)
    cum_row = jnp.dot(decay, upper, precision=HIGHEST, preferred_element_type=f32)
    carry = nt(own_mask.astype(f32), decay, HIGHEST)
    masks, terms = [own_mask], [entry - cum_row]

    for r in range(1, reach + 1):

        @pl.when(g >= r)
        def _(r=r):
            send_table(r).wait_recv()

    behind = jnp.zeros((SUB, 1), f32)
    for r in range(1, reach + 1):
        decay_r = tbuf[r - 1, 0:SUB, :]
        mask_r = doc_col == tbuf[r - 1, 2 * SUB : 2 * SUB + 1, :]
        cum_r = jnp.dot(decay_r, upper, precision=HIGHEST, preferred_element_type=f32)
        total_r = cum_r[:, tokens - 1 : tokens]
        terms.append(tbuf[r - 1, SUB : 2 * SUB, :] + ((total_r - cum_r) + behind))
        behind = behind + total_r
        carry = carry + nt(mask_r.astype(f32), decay_r, HIGHEST)
        masks.append(mask_r)

    for load in loads[8:13]:
        load.wait()

    half = max(1, heads // 2)

    def cell_copies(h):
        view = cell.at[:, pl.ds(pl.multiple_of(j * span + h * HD, 128), HD)]
        return [
            remote(view, view, c_send.at[0], c_recv.at[h // half], {"tp": peer}) for peer in peers
        ]

    for h in range(heads):
        cols = slice(h * HD, (h + 1) * HD)
        for r in range(1, reach + 1):

            @pl.when(g >= r)
            def _(r=r, h=h):
                arrived(kvbuf.at[r - 1, :, :, pl.ds(h * HD, HD)], k_recv.at[r - 1, h], g - r)

            if shared and r == 1:

                @pl.when(hands_on)
                def _(h=h):
                    for copy in hand_on(h):
                        copy.start()

        q_h = query[:, cols]
        keys = [key[:, cols]] + [kvbuf[r, 0, :, cols] for r in range(reach)]
        values = [value[:, cols]] + [kvbuf[r, 1, :, cols] for r in range(reach)]
        peak = carry[:, h : h + 1]
        logs = []
        for mask, term in zip(masks, terms):
            log = jnp.where(mask, cum_col[:, h : h + 1] + term[h : h + 1, :], LOW_LOG)
            peak = jnp.maximum(peak, jnp.max(log, axis=1, keepdims=True))
            logs.append(log)
        denom = jnp.zeros((tokens, 1), f32)
        numer = jnp.zeros((tokens, HD), f32)
        for log, k_b, v_b in zip(logs, keys, values):
            score = nt(q_h, k_b) * (HD ** -0.5) * jnp.exp(log - peak)
            denom = denom + jnp.sum(score, axis=1, keepdims=True)
            numer = numer + jnp.dot(score.astype(bf16), v_b, preferred_element_type=f32)
        value_h = numer / jnp.maximum(jnp.abs(denom), jnp.exp(-peak))
        value_h = value_h * jax.nn.sigmoid(gate_out[:, cols].astype(f32))
        square = jnp.sum(value_h * value_h, axis=1, keepdims=True) * (1.0 / HD)
        value_h = value_h * lax.rsqrt(square + EPSILON) * head_gain[:, cols]
        cell[:, pl.ds(pl.multiple_of(j * span + h * HD, 128), HD)] = value_h.astype(bf16)
        for copy in cell_copies(h):
            copy.start()

    loads[13].wait()
    projected = stream[...].astype(f32)
    for first in range(0, heads, half):
        arrived(cell.at[:, 0 : half * HD * (teams - 1)], c_recv.at[first // half], other)
        for p in range(teams):
            piece = slice(p * span + first * HD, p * span + (first + half) * HD)
            projected = projected + jnp.dot(cell[:, piece], wo[piece, :], preferred_element_type=f32)
    resid[...] = projected.astype(bf16)
    rows_f = resid[...].astype(f32)
    squares = jnp.sum(rows_f * rows_f, axis=1, keepdims=True)
    ssq[j] = jnp.broadcast_to(squares, (tokens, tokens)).T[0:SUB, :]

    def square_copies():
        return [
            remote(ssq.at[j], ssq.at[j], s_send.at[0], s_recv.at[0], {"tp": peer}) for peer in peers
        ]

    for copy in square_copies():
        copy.start()
    normed[...] = (rows_f * row_gain[...].astype(f32).reshape(1, width)).astype(bf16)
    own = pl.ds(pl.multiple_of(g * cap, cap), cap)
    mine = pl.ds(pl.multiple_of(j * width, 128), width)
    block = g // each

    def chunk_of(k):
        if groups != 8:
            return lax.rem(block + k, chunks)
        chip, side = g // 2, lax.rem(g, 2)
        middle = (g >= 2) & (g < 6)

        def picked(order):
            steps = [(step, turn) for step, turn in order if turn < 2 // each]
            at, turn = steps[0]
            for i, (step_i, turn_i) in enumerate(steps[1:]):
                at = jnp.where(k == i + 1, step_i, at)
                turn = jnp.where(k == i + 1, turn_i, turn)
            return at, turn

        at, turn = [jnp.where(middle, mid, end) for mid, end in zip(picked(ORDER_MIDDLE), picked(ORDER_END))]
        pair = chip + 1 - 2 * lax.rem(chip, 2)
        there = jnp.where(
            at == 0, chip, jnp.where(at == 1, pair, jnp.where(at == 2, lax.rem(chip + 2, 4), 3 - chip))
        )
        if each == 2:
            return there
        return 2 * there + lax.rem(side + turn, 2)

    def slot_rows(e):
        return pl.ds(pl.multiple_of(e * cap, cap), cap)

    def dispatch(target):
        return remote(
            packed.at[slot_rows(target)], rows.at[own, mine], z_send.at[0], z_recv.at[g], {"sp": target}
        )

    def give_back(target):
        return remote(
            result.at[slot_rows(target)], returned.at[own], r_send.at[0], r_recv.at[0], {"sp": target}
        )

    def over_others(body):
        def one(k, carry_):
            c = chunk_of(k)
            for p in range(each):
                target = c * each + p

                @pl.when(target != g)
                def _():
                    body(target)

            return carry_

        lax.fori_loop(0, chunks, one, 0)

    lined = groups == 8 and each == 1
    if lined:
        middle = (g >= 2) & (g < 6)
        paces = [jnp.where(middle, mid, end) for mid, end in PACES]
    else:
        paces = [max(-1, k - 3) for k in range(chunks)]

    def issue(now):
        for k, pace in list(enumerate(paces))[early:]:

            @pl.when(pace == now)
            def _(k=k):
                pack_chunk(chunk_of(k))
                send_chunk(chunk_of(k))

    def send_chunk(c):
        for p in range(each):
            target = c * each + p

            @pl.when(target != g)
            def _():
                dispatch(target).start()

    early = 4 if lined else min(chunks, 3)

    def pack_chunk(c):
        at = pl.ds(pl.multiple_of(c * tall, tall), tall)
        packed[at, :] = jnp.dot(chooser[at, :], normed[...], preferred_element_type=f32).astype(bf16)

    def pack(turn, carry_):
        k = jnp.where(turn == 0, 2, jnp.where(turn <= 2, turn - 1, turn)) if lined else turn
        c = chunk_of(k)
        pack_chunk(c)

        @pl.when(k == 0)
        def _():
            rows[own, mine] = packed[own, :]

        send_chunk(c)

        @pl.when(k == 0)
        def _():
            start_spread(c)

        return carry_

    def row_of(c):
        return pl.multiple_of(c * tall, tall)

    def start_spread(c):
        for p in range(each):
            source = c * each + p

            @pl.when(source != g)
            def _():
                place = rows.at[slot_rows(source), mine]
                arrived(place, z_recv.at[source], source)

        for copy in spread_own(teams, j, rows, row_of(c), tall, width, c, t_send, t_recv):
            copy.start()

    def finish(c):
        row = row_of(c)
        relay_arrived(teams, other, hidden, row, tall, hide, c, h_recv)
        result[pl.ds(row, tall), :] = jnp.dot(
            hidden[pl.ds(row, tall), :], down[...], preferred_element_type=f32
        ).astype(bf16)
        for p in range(each):
            target = c * each + p

            @pl.when(target != g)
            def _():
                give_back(target).start()

            @pl.when(target == g)
            def _():
                returned[own, :] = result[own, :]

    def hidden_relay(c):
        row = row_of(c)
        own_arrived(teams, other, hidden, row, tall, hide, c, h_recv)
        for copy in spread_relay(teams, j, hidden, row, tall, hide, c, h_send, h_recv):
            copy.start()

    lax.fori_loop(0, early, pack, 0)
    arrived(ssq.at[0 : teams - 1], s_recv.at[0], other)
    total = ssq[0]
    for p in range(1, teams):
        total = total + ssq[p]
    scale = lax.rsqrt(total * (1.0 / model) + EPSILON)
    slot_scale = nt(scale, chooser[...].astype(f32), HIGHEST)
    for e in range(groups):
        scales[e, :, 0:cap] = slot_scale[:, e * cap : (e + 1) * cap]
    scales_in[g] = scales[g]

    def scale_copy(target):
        return remote(scales.at[target], scales_in.at[g], n_send.at[0], n_recv.at[g], {"sp": target})

    over_others(lambda target: scale_copy(target).start())
    for load in loads[14:]:
        load.wait()

    def stage(k, carry_):
        issue(k)

        @pl.when(k < chunks - 1)
        def _():
            start_spread(chunk_of(k + 1))

        @pl.when(k < chunks)
        def _():
            c = chunk_of(k)
            row = row_of(c)
            own_arrived(teams, other, rows, row, tall, width, c, t_recv)
            for copy in spread_relay(teams, j, rows, row, tall, width, c, t_send, t_recv):
                copy.start()

        @pl.when((k >= 1) & (k < chunks + 1))
        def _():
            c = chunk_of(k - 1)
            row = row_of(c)
            relay_arrived(teams, other, rows, row, tall, width, c, t_recv)
            columns_ = []
            for p in range(each):
                source = c * each + p

                @pl.when(source != g)
                def _():
                    place = scales_in.at[source]
                    arrived(place, n_recv.at[source], source)

                line = scales_in[source][0:1, :]
                columns_.append(jnp.broadcast_to(line, (128, 128)).T[0:cap, 0:1])
            factor = columns_[0] if each == 1 else jnp.concatenate(columns_, axis=0)
            block_rows = rows[pl.ds(row, tall), :]
            opened = jnp.dot(block_rows, gate[...], preferred_element_type=f32) * factor
            raised = jnp.dot(block_rows, up[...], preferred_element_type=f32) * factor
            made = (opened * jax.nn.sigmoid(opened) * raised).astype(bf16)
            hidden[pl.ds(row, tall), pl.ds(pl.multiple_of(j * hide, 128), hide)] = made
            for copy in spread_own(teams, j, hidden, row, tall, hide, c, h_send, h_recv):
                copy.start()

        @pl.when((k >= 2) & (k < chunks + 2))
        def _():
            hidden_relay(chunk_of(k - 2))

        @pl.when(k >= 3)
        def _():
            finish(chunk_of(k - 3))

        return carry_

    lax.fori_loop(0, chunks + 3, stage, 0)

    for r in range(1, reach + 1):

        @pl.when(g + r < groups)
        def _(r=r):
            send_table(r).wait_send()

        @pl.when(sends(r))
        def _(r=r):
            departed(kvbuf.at[r - 1], k_send.at[r - 1], g + r)

    if shared:

        @pl.when(hands_on)
        def _():
            departed(kvbuf.at[0], f_send.at[0], g + 1)

    departed(cell.at[:, 0 : span * (teams - 1)], c_send.at[0], other)
    departed(ssq.at[0 : teams - 1], s_send.at[0], other)
    departed(scales.at[0 : groups - 1], n_send.at[0], other)
    departed(packed.at[0 : (groups - 1) * cap], z_send.at[0], other)
    departed(rows.at[:, 0 : (teams - 1) * width], t_send.at[0], other)
    departed(hidden.at[:, 0 : (teams - 1) * hide], h_send.at[0], other)
    arrived(returned.at[0 : (groups - 1) * cap], r_recv.at[0], other)
    part = width // 2 if width % 256 == 0 else width
    stores = []
    for i in range(width // part):
        cut = slice(i * part, (i + 1) * part)
        mixed = jnp.dot(comb[...], returned[:, cut], preferred_element_type=f32)
        resid[:, cut] = (resid[:, cut].astype(f32) + mixed).astype(bf16)
        stores.append(pltpu.make_async_copy(resid.at[:, cut], out.at[:, cut], o_sem.at[i]))
        stores[-1].start()
    departed(result.at[0 : (groups - 1) * cap], r_send.at[0], other)
    for store in stores:
        store.wait()


def per_device(
    cell_query_heads,
    cell_key_heads,
    cell_value_heads,
    output_gate_logits,
    input_gate_log,
    forget_gate_logits,
    extra_log_decay,
    documents,
    head_norm_gain,
    stream,
    output_weight,
    expert_norm_gain,
    expert_choice_index,
    routing_weight,
    gate_weight,
    up_weight,
    down_weight,
):
    groups, teams = lax.axis_size("sp"), lax.axis_size("tp")
    tokens, heads = input_gate_log.shape
    span = heads * HD
    width = stream.shape[1]
    _, model, hide = gate_weight.shape
    _, hidden_all, _ = down_weight.shape
    experts_all = groups * gate_weight.shape[0]
    cap = 2 * tokens * TOPK // experts_all
    slots = groups * cap
    each = max(1, min(groups, EACH * 64 // cap))
    chunks = groups // each
    reach = max(1, groups // 4)
    arrays = (
        cell_key_heads,
        cell_value_heads,
        forget_gate_logits.T,
        input_gate_log.T,
        extra_log_decay.T,
        documents[None, :],
        expert_choice_index.T,
        routing_weight.T,
        cell_query_heads,
        output_gate_logits,
        head_norm_gain[None, :],
        stream,
        expert_norm_gain,
        output_weight,
        gate_weight,
        up_weight,
        down_weight,
    )
    hbm = pl.BlockSpec(memory_space=pl.ANY)
    dma = pltpu.SemaphoreType.DMA
    return pl.pallas_call(
        functools.partial(kernel, groups, teams, heads, reach, cap, each, chunks),
        out_shape=jax.ShapeDtypeStruct((tokens, width), bf16),
        in_specs=[hbm] * 17,
        out_specs=hbm,
        scratch_shapes=[
            *(pltpu.VMEM(a.shape[-2:], a.dtype) for a in arrays),
            pltpu.VMEM((3 * SUB, tokens), f32),
            pltpu.VMEM((reach, 2, tokens, span), bf16),
            pltpu.VMEM((reach, 3 * SUB, tokens), f32),
            pltpu.VMEM((tokens, teams * span), bf16),
            pltpu.VMEM((teams, SUB, tokens), f32),
            pltpu.VMEM((groups, SUB, 128), f32),
            pltpu.VMEM((groups, SUB, 128), f32),
            pltpu.VMEM((slots, tokens), bf16),
            pltpu.VMEM((tokens, slots), bf16),
            pltpu.VMEM((tokens, width), bf16),
            pltpu.VMEM((tokens, width), bf16),
            pltpu.VMEM((slots, width), bf16),
            pltpu.VMEM((slots, model), bf16),
            pltpu.VMEM((slots, hidden_all), bf16),
            pltpu.VMEM((slots, width), bf16),
            pltpu.VMEM((slots, width), bf16),
            dma((len(arrays),)),
            dma((reach,)),
            dma((reach, heads)),
            dma((1,)),
            dma((reach,)),
            dma((reach,)),
            dma((1,)),
            dma((2,)),
            dma((1,)),
            dma((1,)),
            dma((2,)),
            dma((1,)),
            dma((groups,)),
            dma((1,)),
            dma((groups,)),
            dma((1,)),
            dma((chunks, 2)),
            dma((1,)),
            dma((chunks, 2)),
            dma((1,)),
            dma((1,)),
        ],
        compiler_params=pltpu.CompilerParams(
            collective_id=1, has_side_effects=True, vmem_limit_bytes=VMEM_LIMIT
        ),
    )(*arrays)


def solution(mesh):
    placed = (
        P("sp", "tp"),
        P("sp", "tp"),
        P("sp", "tp"),
        P("sp", "tp"),
        P("sp", "tp"),
        P("sp", "tp"),
        P("sp", "tp"),
        P("sp"),
        P("tp"),
        P("sp", "tp"),
        P(None, "tp"),
        P("tp"),
        P("sp", None),
        P("sp", None),
        P("sp", None, "tp"),
        P("sp", None, "tp"),
        P("sp", None, "tp"),
    )
    return jax.shard_map(
        per_device, mesh=mesh, in_specs=placed, out_specs=P("sp", "tp"), check_vma=False
    )
```
